256 devices in a mesh: sp: 16 (over y, x), dp: 16 (over z, core).
Axes of the slice: x: 4, y: 4, z: 8, core: 2. Of those that a mesh axis runs over, the one named last changes fastest.
Arguments:
- tokens: bfloat16 [16, 5120, 2048], P('dp', 'sp'), may hold values from -6 to 6
- up_weight: bfloat16 [2048, 2048], P('dp'), may hold values from -0.125 to 0.125
- gate_weight: bfloat16 [2048, 2048], P('dp'), may hold values from -0.125 to 0.125
- group_gain: float32 [16, 128], P('sp'), may hold values from 0.1 to 1.9
- mix_weight: bfloat16 [16, 1280, 1280], P('sp', 'dp'), may hold values from -0.15625 to 0.15625
- mix_bias: float32 [16, 1280], P('sp'), may hold values from 0.5 to 1.5
- out_gain: float32 [2048], replicated, may hold values from 0.1 to 1.9
- out_weight: bfloat16 [2048, 2048], P(None, 'dp'), may hold values from -0.125 to 0.125
Outputs:
- mixed_out: bfloat16 [16, 5120, 2048], P('dp', 'sp')
The draws below stay inside these ranges and needn't reach their ends.
All inputs are finite; a program needn't handle non-finite values.
Results may differ from the reference program's by a relative error of at most 0.0072.
Values may be sent and summed in bfloat16 or wider, within the bound.
A program may use at most 128 MiB of HBM per device.

```python
import jax
import jax.numpy as jnp
from jax import lax

D = 2048
GROUPS = 16
GROUP_DIM = 128
SPAN = 1280
WIDTH = 2048
LENGTH = 5120
SEQS = 16


def level_of(key, extent, cuts, smallest, top_value):
    level, own = 1.0, jax.random.fold_in(key, 6)
    for axis_at, parts in cuts:
        steps = jnp.exp(jax.random.uniform(jax.random.fold_in(own, axis_at), (parts,), jnp.float32, smallest / len(cuts), top_value / len(cuts)))
        level = level * jnp.repeat(steps, extent[axis_at] // parts).reshape([-1 if axis == axis_at else 1 for axis in range(len(extent))])
    return level


def normal_values(own_key, dims, deviation, most, cuts=(), held_as=jnp.bfloat16):
    entries = deviation * jax.random.normal(own_key, dims, jnp.float32)
    if cuts:
        entries = entries * level_of(own_key, dims, cuts, -0.22, 0.18)
    return jnp.clip(entries, -most, most).astype(held_as)


def setup_inputs(seed: int = 0) -> dict:
    splits = jax.random.split(jax.random.key(seed), 9)
    tokens = normal_values(splits[0], (SEQS, LENGTH, D), 1.0, 6.0, ((0, 16), (1, 16)))
    up_weight = normal_values(splits[1], (D, WIDTH), D ** -0.5, 0.125, ((0, 16),))
    gate_weight = normal_values(splits[2], (D, WIDTH), D ** -0.5, 0.125, ((0, 16),))
    group_gain = jnp.clip(1.0 + 0.18 * jax.random.normal(splits[3], (GROUPS, GROUP_DIM), jnp.float32), 0.1, 1.9)
    mix_weight = normal_values(splits[4], (GROUPS, SPAN, SPAN), SPAN ** -0.5, 0.15625, ((0, 16), (1, 16)))
    mix_bias = jnp.clip(0.5 + 1.0 * jax.random.uniform(splits[5], (GROUPS, SPAN), jnp.float32) ** level_of(splits[5], (GROUPS, SPAN), ((0, 16),), -0.2, 0.2), 0.5, 1.5)
    out_gain = jnp.clip(1.0 + 0.18 * jax.random.normal(splits[6], (WIDTH,), jnp.float32), 0.1, 1.9)
    out_weight = normal_values(splits[7], (WIDTH, D), WIDTH ** -0.5, 0.125, ((1, 16),))
    return {"tokens": tokens, "up_weight": up_weight, "gate_weight": gate_weight, "group_gain": group_gain, "mix_weight": mix_weight, "mix_bias": mix_bias, "out_gain": out_gain, "out_weight": out_weight}


norm_eps = 1e-06

def reference(tokens, up_weight, gate_weight, group_gain, mix_weight, mix_bias, out_gain, out_weight):
    lower = jnp.tril(jnp.ones((SPAN, SPAN), dtype=bool))
    mix_mask = jnp.where(lower[None], mix_weight, jnp.zeros_like(mix_weight)).astype(jnp.float32)
    bias_cols = mix_bias.astype(jnp.float32).T

    def one_sequence(sequence):
        up_proj = jnp.dot(sequence, up_weight, preferred_element_type=jnp.float32).astype(jnp.bfloat16)
        gate_proj = jnp.dot(sequence, gate_weight, preferred_element_type=jnp.float32).astype(jnp.bfloat16)
        up_proj = lax.optimization_barrier(up_proj)
        gate_proj = lax.optimization_barrier(gate_proj)
        opened = jax.nn.gelu(up_proj.astype(jnp.float32)).reshape(LENGTH, GROUPS, GROUP_DIM)
        gate_act = jax.nn.gelu(gate_proj.astype(jnp.float32)).reshape(LENGTH, GROUPS, GROUP_DIM)
        center = lax.optimization_barrier(jnp.mean(gate_act, axis=-1, keepdims=True))
        spread = lax.optimization_barrier(jnp.mean(jnp.square(gate_act - center), axis=-1, keepdims=True))
        normal_v = ((gate_act - center) * lax.rsqrt(spread + norm_eps) * group_gain.astype(jnp.float32)).astype(jnp.bfloat16)
        normal_v = lax.optimization_barrier(normal_v)
        blocks = normal_v.astype(jnp.float32).reshape(LENGTH // SPAN, SPAN, GROUPS, GROUP_DIM)
        mixed_sum = jnp.einsum('gij,njgc->nigc', mix_mask, blocks) + bias_cols[None, :, :, None]
        gated = (opened * mixed_sum.reshape(LENGTH, GROUPS, GROUP_DIM)).astype(jnp.bfloat16)
        gated = lax.optimization_barrier(gated)
        gated_f = gated.astype(jnp.float32).reshape(LENGTH, WIDTH)
        scale = lax.rsqrt(lax.optimization_barrier(jnp.mean(gated_f * gated_f, axis=-1, keepdims=True)) + norm_eps)
        normed = (gated_f * scale * out_gain.astype(jnp.float32)).astype(jnp.bfloat16)
        return jnp.dot(normed, out_weight, preferred_element_type=jnp.float32).astype(jnp.bfloat16)
    return lax.map(one_sequence, tokens)
```

```python
import functools

import jax
import jax.numpy as jnp
from jax import lax
from jax.experimental import pallas as pl
from jax.experimental.pallas import tpu as pltpu
from jax.sharding import PartitionSpec as P

norm_eps = 1e-06
NX, NY, NZ = 4, 4, 8
ROWS = 320
SPAN = 1280
WIDTH = 2048
GD = 128
MROWS = 80
f32 = jnp.float32
bf16 = jnp.bfloat16


def remote(src, dst, send, recv, dev):
    return pltpu.make_async_remote_copy(
        src_ref=src,
        dst_ref=dst,
        send_sem=send,
        recv_sem=recv,
        device_id=dev,
        device_id_type=pl.DeviceIdType.MESH,
    )


def gelu(a):
    return 0.5 * a * (1.0 + jnp.tanh(0.7978845608028654 * (a + 0.044715 * (a * a * a))))


def kernel(
    tokens, upw, gatew, gain, mixw, bias, ogain, outw, out_ref,
    tok, wb, mb, ob, v, op, bt, g, ab, nb, sb, sg,
    lsem, xsend, xrecv, zmsend, zmrecv, zwsend, zwrecv, zosend, zorecv,
    ysend, yrecv, bmsend, bmrecv, bwsend, bwrecv, bosend, borecv,
    asend, arecv, ssend, srecv, asem,
):
    sp = lax.axis_index("sp")
    dp = lax.axis_index("dp")
    y, x = lax.div(sp, NX), lax.rem(sp, NX)
    z, c = lax.div(dp, 2), lax.rem(dp, 2)

    def dev(xx, yy, zz, cc):
        return {"sp": yy * NX + xx, "dp": zz * 2 + cc}

    def mod(a, n):
        return lax.rem(a, n)

    nextx = dev(mod(x + 1 + 2 * c, NX), y, z, c)
    nexty = dev(x, mod(y + 1 + 2 * c, NY), z, c)
    nextz = dev(x, y, mod(z + 1 + 6 * c, NZ), c)
    sib = dev(x, y, z, 1 - c)

    def xat(h):
        return mod(x + h * (3 - 2 * c), NX)

    def yat(h, cc):
        return mod(y + h * (3 - 2 * cc), NY)

    def zat(t, cc):
        return mod(z + t * (7 - 6 * cc), NZ)

    d = z * 2 + c
    loads = [
        pltpu.make_async_copy(tokens.at[0], tok.at[x], lsem.at[0]),
        pltpu.make_async_copy(
            mixw.at[0], mb.at[y, pl.ds(pl.multiple_of(d * MROWS, 16), MROWS), :], lsem.at[1]
        ),
        pltpu.make_async_copy(
            outw, ob.at[:, pl.ds(pl.multiple_of(d * GD, GD), GD)], lsem.at[2]
        ),
        pltpu.make_async_copy(bias, sb.at[y], lsem.at[3]),
        pltpu.make_async_copy(gain, sg.at[y], lsem.at[4]),
    ]
    wrow = pl.ds(pl.multiple_of(d * GD, GD), GD)
    for j in range(4):
        cols = pl.ds(pl.multiple_of((x + 4 * j) * GD, GD), GD)
        loads.append(
            pltpu.make_async_copy(upw.at[:, cols], wb.at[wrow, pl.ds(j * GD, GD)], lsem.at[5 + j])
        )
        loads.append(
            pltpu.make_async_copy(
                gatew.at[:, cols], wb.at[wrow, pl.ds(512 + j * GD, GD)], lsem.at[9 + j]
            )
        )
    for load in loads:
        load.start()

    barrier = pltpu.get_barrier_semaphore()
    peers = [dev(mod(x + k, NX), y, z, c) for k in (1, 2, 3)]
    peers += [dev(x, mod(y + k, NY), z, c) for k in (1, 2, 3)]
    peers += [dev(x, y, mod(z + k, NZ), c) for k in (1, NZ - 1)]
    peers += [sib]
    for peer in peers:
        pl.semaphore_signal(barrier, inc=1, device_id=peer, device_id_type=pl.DeviceIdType.MESH)
    pl.semaphore_wait(barrier, len(peers))
    for load in loads:
        load.wait()

    def xcopy(i):
        hop, k = lax.div(i, 4), lax.rem(i, 4)
        slot = tok.at[xat(hop), pl.ds(pl.multiple_of(k * 80, 16), 80), :]
        return remote(slot, slot, xsend.at[i], xrecv.at[i], nextx)

    def xarrival(i):
        hop, k = lax.div(i, 4), lax.rem(i, 4)
        slot = tok.at[xat(hop + 1), pl.ds(pl.multiple_of(k * 80, 16), 80), :]
        return remote(slot, slot, xsend.at[i], xrecv.at[i], nextx)

    def xservice(i, forward):
        xarrival(i).wait_recv()
        if forward:
            xcopy(i + 4).start()

    def by_width(dd, fn):
        n = lax.div(MROWS * (dd + 1) + 255, 256)
        for k in range(1, 6):
            @pl.when(n == k)
            def _():
                fn(256 * k)

    def mslot(group, dd, width):
        return mb.at[group, pl.ds(pl.multiple_of(dd * MROWS, 16), MROWS), pl.ds(0, width)]

    def mservice(t, arrived):
        dd = zat(t, c) * 2 + c

        def go(width):
            slot = mslot(y, dd, width)
            if arrived:
                remote(slot, slot, zmsend.at[t - 1], zmrecv.at[t - 1], nextz).wait_recv()

            @pl.when(t < NZ - 1)
            def _():
                remote(slot, slot, zmsend.at[t], zmrecv.at[t], nextz).start()

            remote(slot, slot, ysend.at[t], yrecv.at[t], nexty).start()
            remote(slot, slot, bmsend.at[t], bmrecv.at[t], sib).start()

        by_width(dd, go)

    def yservice(h, s):
        dd = zat(s, c) * 2 + c

        def go(width):
            slot = mslot(yat(h + 1, c), dd, width)
            i = h * 8 + s
            remote(slot, slot, ysend.at[i], yrecv.at[i], nexty).wait_recv()
            if h < 2:
                remote(slot, slot, ysend.at[i + 8], yrecv.at[i + 8], nexty).start()
            remote(slot, slot, bmsend.at[i + 8], bmrecv.at[i + 8], sib).start()

        by_width(dd, go)

    def yround(t):
        for h in range(3):
            s = t - 1 - h

            @pl.when((s >= 0) & (s < 8))
            def _():
                yservice(h, s)

    def wslot(t, half, cc):
        dd = zat(t, cc) * 2 + cc
        return wb.at[
            pl.ds(pl.multiple_of(dd * GD, GD), GD), pl.ds(512 * half, 512)
        ]

    def wservice(t, half, arrived):
        slot = wslot(t, half, c)
        if arrived:
            i = (t - 1) * 2 + half
            remote(slot, slot, zwsend.at[i], zwrecv.at[i], nextz).wait_recv()

        @pl.when(t < NZ - 1)
        def _():
            i = t * 2 + half
            remote(slot, slot, zwsend.at[i], zwrecv.at[i], nextz).start()

        i = t * 2 + half
        remote(slot, slot, bwsend.at[i], bwrecv.at[i], sib).start()

    def oslot(t, q, cc):
        dd = zat(t, cc) * 2 + cc
        return ob.at[pl.ds(512 * q, 512), pl.ds(pl.multiple_of(dd * GD, GD), GD)]

    def ofull(t, cc):
        dd = zat(t, cc) * 2 + cc
        return ob.at[:, pl.ds(pl.multiple_of(dd * GD, GD), GD)]

    def oservice(t):
        for q in range(4):
            slot = oslot(t, q, c)
            if t > 0:
                i = (t - 1) * 4 + q
                remote(slot, slot, zosend.at[i], zorecv.at[i], nextz).wait_recv()
            if t < NZ - 1:
                i = t * 4 + q
                remote(slot, slot, zosend.at[i], zorecv.at[i], nextz).start()
        slot = ofull(t, c)
        remote(slot, slot, bosend.at[t], borecv.at[t], sib).start()

    for k in (1, 2, 3):
        peer = dev(x, mod(y + k, NY), z, c)
        remote(sb.at[y], sb.at[y], ssend.at[k - 1], srecv.at[k - 1], peer).start()
        remote(sg.at[y], sg.at[y], ssend.at[k + 2], srecv.at[k + 2], peer).start()
    mservice(0, False)
    for i in range(4):
        xcopy(i).start()
    wservice(0, 0, False)
    wservice(0, 1, False)

    def round_(t, _):
        mservice(t, True)
        yround(t)
        wservice(t, 0, True)
        xservice(t - 1, True)
        wservice(t, 1, True)

        return 0

    lax.fori_loop(1, NZ - 1, round_, 0)
    oservice(0)
    lax.fori_loop(NZ - 1, NZ, round_, 0)

    for t in range(NZ):
        for half in range(2):
            slot = wslot(t, half, 1 - c)
            remote(slot, slot, bwsend.at[2 * t + half], bwrecv.at[2 * t + half], sib).wait_recv()
    for k in (1, 2, 3):
        src = mod(y + NY - k, NY)
        peer = dev(x, src, z, c)
        remote(sb.at[src], sb.at[src], ssend.at[k - 1], srecv.at[k - 1], peer).wait_recv()
        remote(sg.at[src], sg.at[src], ssend.at[k + 2], srecv.at[k + 2], peer).wait_recv()

    def project(xs, r0, n):
        start = pl.multiple_of(xs * ROWS + r0, 16)

        def pair(jj, _):
            t = tok[xs, pl.ds(pl.multiple_of(r0, 16), n), :]
            up = jnp.dot(
                t, wb[:, pl.ds(pl.multiple_of(jj * 256, 256), 256)], preferred_element_type=f32
            )
            gate = jnp.dot(
                t,
                wb[:, pl.ds(pl.multiple_of(512 + jj * 256, 256), 256)],
                preferred_element_type=f32,
            )
            for i in range(2):
                j = 2 * jj + i
                u = up[:, i * GD:(i + 1) * GD].astype(bf16).astype(f32)
                op[j, pl.ds(start, n), :] = gelu(u)
                a = gelu(gate[:, i * GD:(i + 1) * GD].astype(bf16).astype(f32))
                a = a - jnp.mean(a, axis=-1, keepdims=True)
                spread = jnp.mean(a * a, axis=-1, keepdims=True)
                v[j, pl.ds(start, n), :] = (
                    a * lax.rsqrt(spread + norm_eps) * sg[j]
                ).astype(bf16)
            return 0

        lax.fori_loop(0, 2, pair, 0)

    def project_shard(h):
        xs = xat(h)

        def half(i, _):
            project(xs, i * 160, 160)
            return 0

        lax.fori_loop(0, 2, half, 0)

    def spread_bias(j, _):
        bt[j] = jnp.transpose(jnp.broadcast_to(sb[j], (GD, SPAN)))
        return 0

    project_shard(0)
    yround(8)
    project_shard(1)
    xservice(7, True)
    oservice(1)
    yround(9)
    project_shard(2)
    yround(10)
    lax.fori_loop(0, 4, spread_bias, 0)
    oservice(2)

    for i in range(8, 12):
        xservice(i, False)
        project(xat(3), (i - 8) * 80, 80)

    for h in range(4):
        def msib(t, _):
            dd = zat(t, 1 - c) * 2 + 1 - c

            def go(width):
                slot = mslot(yat(h, 1 - c), dd, width)
                i = h * 8 + t
                remote(slot, slot, bmsend.at[i], bmrecv.at[i], sib).wait_recv()

            by_width(dd, go)
            return 0

        lax.fori_loop(0, 8, msib, 0)

    kmax = (384, 640, 1024, 1280)
    kfree = (0, 256, 640, 896)

    def acopy(j, r):
        lanes = pl.ds(pl.multiple_of((4 * j + x) * GD, GD), GD)
        src = g.at[j, pl.ds(ROWS * r, ROWS), :]
        return remote(src, ab.at[:, lanes], asend.at[r * 4 + j], arecv.at[x * 4 + j], dev(r, y, z, c))

    def alocal(j, r):
        lanes = pl.ds(pl.multiple_of((4 * j + x) * GD, GD), GD)
        src = g.at[j, pl.ds(ROWS * r, ROWS), :]
        return pltpu.make_async_copy(src, ab.at[:, lanes], asem.at[j])

    def mix(j, _):
        for r in range(4):
            rows = pl.ds(ROWS * r, ROWS)
            k0, k1 = kfree[r], kmax[r]
            at_row = lax.broadcasted_iota(jnp.int32, (ROWS, k1 - k0), 0) + ROWS * r
            at_col = lax.broadcasted_iota(jnp.int32, (ROWS, k1 - k0), 1) + k0
            edge = mb[j, rows, k0:k1].astype(f32)
            edge = jnp.where(at_col <= at_row, edge, 0.0).astype(bf16)
            total = jnp.dot(edge, v[j, k0:k1, :], preferred_element_type=f32)
            if k0:
                total += jnp.dot(
                    mb[j, rows, 0:k0], v[j, 0:k0, :], preferred_element_type=f32
                )
            g[j, rows, :] = (op[j, rows, :] * (total + bt[j, rows, :])).astype(bf16)

            @pl.when(x != r)
            def _():
                acopy(j, r).start()

            @pl.when(x == r)
            def _():
                alocal(j, r).start()
        return 0

    lax.fori_loop(0, 4, mix, 0)
    oservice(3)
    oservice(4)

    def await_gated(j, _):
        for k in (1, 2, 3):
            src = mod(x + k, NX)
            lanes = pl.ds(pl.multiple_of((4 * j + src) * GD, GD), GD)
            slot = ab.at[:, lanes]
            remote(slot, slot, asend.at[0], arecv.at[src * 4 + j], sib).wait_recv()
        for r in range(4):
            @pl.when(x == r)
            def _():
                alocal(j, r).wait()
        return 0

    lax.fori_loop(0, 4, await_gated, 0)

    def rms(i, _):
        rows = pl.ds(pl.multiple_of(i * 16, 16), 16)
        a = ab[rows, :].astype(f32)
        scale = lax.rsqrt(jnp.mean(a * a, axis=-1, keepdims=True) + norm_eps)
        nb[rows, :] = (a * scale * ogain[...]).astype(bf16)
        return 0

    lax.fori_loop(0, ROWS // 16, rms, 0)
    oservice(5)

    def osib(t):
        slot = ofull(t, 1 - c)
        remote(slot, slot, bosend.at[t], borecv.at[t], sib).wait_recv()

    def emit(zz):
        cols = pl.ds(pl.multiple_of(zz * 256, 256), 256)
        out_ref[0, :, cols] = jnp.dot(nb[...], ob[:, cols], preferred_element_type=f32).astype(bf16)

    for t in range(6):
        osib(t)
    for k in (0, 4, 3, 5):
        emit(mod(z + k, NZ))
    for t in (6, 7):
        oservice(t)
        osib(t)
        emit(mod(z + 8 - t, NZ))
        emit(mod(z + t, NZ))

    for k in (1, 2, 3):
        remote(sb.at[y], sb.at[y], ssend.at[k - 1], srecv.at[k - 1], sib).wait_send()
        remote(sg.at[y], sg.at[y], ssend.at[k + 2], srecv.at[k + 2], sib).wait_send()

    def xsent(i, _):
        xcopy(i).wait_send()
        return 0

    lax.fori_loop(0, 12, xsent, 0)

    def msent(t, _):
        dd = zat(t, c) * 2 + c

        def go(width):
            slot = mslot(y, dd, width)

            @pl.when(t < NZ - 1)
            def _():
                remote(slot, slot, zmsend.at[t], zmrecv.at[t], nextz).wait_send()

            for h in range(4):
                i = h * 8 + t
                if h < 3:
                    remote(slot, slot, ysend.at[i], yrecv.at[i], nexty).wait_send()
                remote(slot, slot, bmsend.at[i], bmrecv.at[i], sib).wait_send()

        by_width(dd, go)

        for half in range(2):
            slot = wslot(t, half, c)
            i = t * 2 + half

            @pl.when(t < NZ - 1)
            def _():
                remote(slot, slot, zwsend.at[i], zwrecv.at[i], nextz).wait_send()

            remote(slot, slot, bwsend.at[i], bwrecv.at[i], sib).wait_send()

        @pl.when(t < NZ - 1)
        def _():
            for q in range(4):
                slot = oslot(t, q, c)
                remote(slot, slot, zosend.at[t * 4 + q], zorecv.at[t * 4 + q], nextz).wait_send()

        slot = ofull(t, c)
        remote(slot, slot, bosend.at[t], borecv.at[t], sib).wait_send()
        return 0

    lax.fori_loop(0, 8, msent, 0)

    def asent(j, _):
        for r in range(4):
            @pl.when(x != r)
            def _():
                acopy(j, r).wait_send()
        return 0

    lax.fori_loop(0, 4, asent, 0)


def body(tokens, up_weight, gate_weight, group_gain, mix_weight, mix_bias, out_gain, out_weight):
    hbm = pl.BlockSpec(memory_space=pl.ANY)
    vmem = pl.BlockSpec(memory_space=pltpu.VMEM)
    dma = pltpu.SemaphoreType.DMA
    return pl.pallas_call(
        kernel,
        out_shape=jax.ShapeDtypeStruct((1, ROWS, WIDTH), bf16),
        in_specs=[hbm, hbm, hbm, hbm, hbm, hbm, vmem, hbm],
        out_specs=vmem,
        scratch_shapes=[
            pltpu.VMEM((NX, ROWS, WIDTH), bf16),
            pltpu.VMEM((WIDTH, 1024), bf16),
            pltpu.VMEM((4, SPAN, SPAN), bf16),
            pltpu.VMEM((WIDTH, WIDTH), bf16),
            pltpu.VMEM((4, SPAN, GD), bf16),
            pltpu.VMEM((4, SPAN, GD), f32),
            pltpu.VMEM((4, SPAN, GD), f32),
            pltpu.VMEM((4, SPAN, GD), bf16),
            pltpu.VMEM((ROWS, WIDTH), bf16),
            pltpu.VMEM((ROWS, WIDTH), bf16),
            pltpu.VMEM((4, 1, SPAN), f32),
            pltpu.VMEM((4, 1, GD), f32),
            dma((13,)),
            dma((12,)), dma((12,)),
            dma((7,)), dma((7,)),
            dma((14,)), dma((14,)),
            dma((28,)), dma((28,)),
            dma((24,)), dma((24,)),
            dma((32,)), dma((32,)),
            dma((16,)), dma((16,)),
            dma((8,)), dma((8,)),
            dma((16,)), dma((16,)),
            dma((6,)), dma((6,)),
            dma((4,)),
        ],
        compiler_params=pltpu.CompilerParams(
            collective_id=0, has_side_effects=True, vmem_limit_bytes=66_000_000
        ),
        name="gating",
    )(
        tokens, up_weight, gate_weight, group_gain, mix_weight, mix_bias,
        out_gain.reshape(1, WIDTH), out_weight,
    )


def solution(mesh):
    return jax.shard_map(
        body,
        mesh=mesh,
        in_specs=(
            P("dp", "sp", None),
            P("dp", None),
            P("dp", None),
            P("sp", None),
            P("sp", "dp", None),
            P("sp", None),
            P(),
            P(None, "dp"),
        ),
        out_specs=P("dp", "sp", None),
        check_vma=False,
    )
```

```python
import functools

import jax
import jax.numpy as jnp
from jax import lax
from jax.experimental import pallas as pl
from jax.experimental.pallas import tpu as pltpu
from jax.sharding import PartitionSpec as P

norm_eps = 1e-06
NX, NY, NZ = 4, 4, 8
ROWS = 320
SPAN = 1280
WIDTH = 2048
GD = 128
MROWS = 80
OZ = 1024
OQ = (WIDTH - OZ) // 4
XN = 4
XR = ROWS // XN
MSUM = (352, 384)
f32 = jnp.float32
bf16 = jnp.bfloat16


def remote(src, dst, send, recv, dev):
    return pltpu.make_async_remote_copy(
        src_ref=src,
        dst_ref=dst,
        send_sem=send,
        recv_sem=recv,
        device_id=dev,
        device_id_type=pl.DeviceIdType.MESH,
    )


def gelu(a):
    return 0.5 * a * (1.0 + jnp.tanh(0.7978845608028654 * (a + 0.044715 * (a * a * a))))


def kernel(
    tokens, upw, gatew, gain, mixw, bias, ogain, outw, out_ref,
    tok, wb, mb, ob, v, op, bt, g, ab, nb, sb, sg,
    lsem, xsend, xrecv, zmsend, zmrecv, zwsend, zwrecv, zqsend, zqrecv,
    zpsend, zprecv, ysend, yrecv, oysend, oyrecv, bsend, brecv,
    asend, arecv, ssend, srecv, asem,
):
    sp = lax.axis_index("sp")
    dp = lax.axis_index("dp")
    y, x = lax.div(sp, NX), lax.rem(sp, NX)
    z, c = lax.div(dp, 2), lax.rem(dp, 2)

    def dev(xx, yy, zz, cc):
        return {"sp": yy * NX + xx, "dp": zz * 2 + cc}

    def mod(a, n):
        return lax.rem(a, n)

    tox = [dev(mod(x + 1, NX), y, z, c), dev(mod(x + NX - 1, NX), y, z, c)]
    toy = [dev(x, mod(y + 1, NY), z, c), dev(x, mod(y + NY - 1, NY), z, c)]
    toz = [dev(x, y, mod(z + 1, NZ), c), dev(x, y, mod(z + NZ - 1, NZ), c)]
    sib = dev(x, y, z, 1 - c)

    def xorg(r, way):
        return mod(x + (NX - r if way == 0 else r), NX)

    def yorg(r, way):
        return mod(y + (NY - r if way == 0 else r), NY)

    def zorg(r, way):
        return mod(z + (NZ - r if way == 0 else r), NZ)

    d = z * 2 + c
    wrow = pl.ds(pl.multiple_of(d * GD, GD), GD)
    loads = [
        pltpu.make_async_copy(
            mixw.at[0], mb.at[y, pl.ds(pl.multiple_of(d * MROWS, 16), MROWS), :], lsem.at[1]
        ),
        pltpu.make_async_copy(tokens.at[0], tok.at[x], lsem.at[0]),
        pltpu.make_async_copy(outw, ob.at[:, wrow], lsem.at[2]),
        pltpu.make_async_copy(bias, sb.at[y], lsem.at[3]),
        pltpu.make_async_copy(gain, sg.at[y], lsem.at[4]),
    ]
    for load in loads:
        load.start()
    for j in range(4):
        cols = pl.ds(pl.multiple_of((x + 4 * j) * GD, GD), GD)
        for half, w in enumerate((upw, gatew)):
            pltpu.make_async_copy(
                w.at[:, cols], wb.at[wrow, pl.ds(512 * half + j * GD, GD)], lsem.at[5]
            ).start()
    loads.append(pltpu.make_async_copy(wb.at[wrow, :], wb.at[wrow, :], lsem.at[5]))

    barrier = pltpu.get_barrier_semaphore()
    peers = [dev(mod(x + k, NX), y, z, c) for k in (1, 2, 3)]
    peers += [dev(x, mod(y + k, NY), z, c) for k in (1, 2, 3)]
    peers += toz + [sib]
    for peer in peers:
        pl.semaphore_signal(barrier, inc=1, device_id=peer, device_id_type=pl.DeviceIdType.MESH)
    pl.semaphore_wait(barrier, len(peers))
    for load in loads:
        load.wait()

    def xslot(shard, k):
        return tok.at[shard, pl.ds(k * XR, XR), :]

    xfrom1 = mod(x + NX - 1 + 2 * c, NX)
    xfrom2 = mod(x + 2, NX)
    xto = dev(mod(x + 1 + 2 * c, NX), y, z, c)

    def xforward(k):
        slot = xslot(xfrom1, k)
        remote(slot, slot, xsend.at[0], xrecv.at[c * XN + k], xto).wait_recv()
        remote(slot, slot, xsend.at[0], xrecv.at[2 * XN + k], xto).start()

    def by_width(dd, fn):
        n = lax.div(MROWS * (dd + 1) + GD - 1, GD)
        for k in range(1, 11):
            @pl.when(n == k)
            def _():
                fn(GD * k)

    def mslot(group, dd, width):
        return mb.at[group, pl.ds(pl.multiple_of(dd * MROWS, 16), MROWS), pl.ds(0, width)]

    def steps(r, way):
        if r == 0:
            return z, None, [0, 1], 0
        if r == 4:
            return mod(z + 4, NZ), 6 + c, [], 7
        return zorg(r, way), (r - 1) * 2 + way, [way], 2 * r - 1 + way

    def onward(r, way, start):
        for w in way:
            if r < 3:
                start(w)
            else:
                @pl.when(c == w)
                def _():
                    start(w)

    def mstep(r, way=None):
        org, at, ways, k = steps(r, way)
        dd = org * 2 + c

        def go(width):
            slot = mslot(y, dd, width)
            if at is not None:
                remote(slot, slot, zmsend.at[0], zmrecv.at[at], sib).wait_recv()

            def start(w):
                i = r * 2 + w
                remote(slot, slot, zmsend.at[i], zmrecv.at[i], toz[w]).start()

            onward(r, ways, start)
            for w in range(2):
                remote(slot, slot, ysend.at[0], yrecv.at[w * 8 + k], toy[w]).start()
            remote(slot, slot, bsend.at[0], brecv.at[0], sib).start()

        by_width(dd, go)

    def ygroup(a):
        return mod(y + 2, NY) if a == 2 else yorg(1, a)

    def kchip(k):
        if k == 0:
            return z
        if k == 7:
            return mod(z + 4, NZ)
        return zorg((k + 1) // 2, (k + 1) % 2)

    def ystep(a, k):
        dd = kchip(k) * 2 + c

        def go(width):
            slot = mslot(ygroup(a), dd, width)
            remote(slot, slot, ysend.at[0], yrecv.at[a * 8 + k], sib).wait_recv()
            if a < 2:
                @pl.when(c == a)
                def _():
                    remote(slot, slot, ysend.at[0], yrecv.at[16 + k], toy[a]).start()
            remote(slot, slot, bsend.at[0], brecv.at[0], sib).start()

        by_width(dd, go)

    def wstep(r, half, way=None):
        org, at, ways, k = steps(r, way)
        slot = wb.at[
            pl.ds(pl.multiple_of((org * 2 + c) * GD, GD), GD), pl.ds(512 * half, 512)
        ]
        if at is not None:
            remote(slot, slot, zwsend.at[0], zwrecv.at[at * 2 + half], sib).wait_recv()

        def start(w):
            i = (r * 2 + w) * 2 + half
            remote(slot, slot, zwsend.at[0], zwrecv.at[i], toz[w]).start()

        onward(r, ways, start)
        remote(slot, slot, bsend.at[1], brecv.at[1], sib).start()

    def qstep(r, half, way=None):
        org, at, ways, k = steps(r, way)
        slot = ob.at[
            pl.ds(OZ // 2 * half, OZ // 2), pl.ds(pl.multiple_of((org * 2 + c) * GD, GD), GD)
        ]
        if at is not None:
            remote(slot, slot, zqsend.at[0], zqrecv.at[at * 2 + half], sib).wait_recv()

        def start(w):
            i = (r * 2 + w) * 2 + half
            remote(slot, slot, zqsend.at[0], zqrecv.at[i], toz[w]).start()

        onward(r, ways, start)
        remote(slot, slot, bsend.at[2], brecv.at[2], sib).start()

    def pslot(group, chip):
        rows = pl.ds(pl.multiple_of(OZ + OQ * group, 16), OQ)
        return ob.at[rows, pl.ds(pl.multiple_of((chip * 2 + c) * GD, GD), GD)]

    def pstep(r, way=None):
        org, at, ways, k = steps(r, way)
        slot = pslot(y, org)
        if at is not None:
            remote(slot, slot, zpsend.at[0], zprecv.at[at], sib).wait_recv()

        def start(w):
            i = r * 2 + w
            remote(slot, slot, zpsend.at[0], zprecv.at[i], toz[w]).start()

        onward(r, ways, start)
        for w in range(2):
            remote(slot, slot, oysend.at[0], oyrecv.at[w * 8 + k], toy[w]).start()
        remote(slot, slot, bsend.at[3], brecv.at[3], sib).start()

    def pystep(a, k):
        slot = pslot(ygroup(a), kchip(k))
        remote(slot, slot, oysend.at[0], oyrecv.at[a * 8 + k], sib).wait_recv()
        if a < 2:
            @pl.when(c == a)
            def _():
                remote(slot, slot, oysend.at[0], oyrecv.at[16 + k], toy[a]).start()
        remote(slot, slot, bsend.at[3], brecv.at[3], sib).start()

    def yrun(fn, ks, ways):
        for k in ks:
            for a in ways:
                fn(a, k)

    def mpair(r):
        mstep(r, 0)
        mstep(r, 1)

    def wpair(r):
        for half in range(2):
            wstep(r, half, 0)
            wstep(r, half, 1)

    def qpair(r):
        for half in range(2):
            qstep(r, half, 0)
            qstep(r, half, 1)

    def ppair(r):
        pstep(r, 0)
        pstep(r, 1)

    mstep(0)
    for k in range(XN):
        for w in range(2):
            remote(xslot(x, k), xslot(x, k), xsend.at[0], xrecv.at[w * XN + k], tox[w]).start()
    wstep(0, 0)
    wstep(0, 1)
    for k in (1, 2, 3):
        peer = dev(x, mod(y + k, NY), z, c)
        remote(sb.at[y], sb.at[y], ssend.at[0], srecv.at[0], peer).start()
        remote(sg.at[y], sg.at[y], ssend.at[1], srecv.at[1], peer).start()

    mpair(1)
    wpair(1)
    mpair(2)
    yrun(ystep, (0,), (0, 1, 2))
    wpair(2)
    xforward(0)
    yrun(ystep, (1, 2), (0, 1))
    mpair(3)
    yrun(ystep, (1, 2), (2,))
    xforward(1)
    yrun(ystep, (3, 4), (0, 1))
    wpair(3)
    pstep(0)
    qstep(0, 0)
    qstep(0, 1)
    xforward(2)
    mstep(4)
    yrun(ystep, (3, 4), (2,))
    yrun(ystep, (5, 6), (0, 1))
    wstep(4, 0)
    wstep(4, 1)
    xforward(3)
    ppair(1)

    def wait_all(ref, i):
        remote(ref, ref, bsend.at[i], brecv.at[i], sib).wait_recv()

    wait_all(wb.at[0:1024, :], 1)
    remote(sb.at[0:3], sb.at[0:3], ssend.at[0], srecv.at[0], sib).wait_recv()
    remote(sg.at[0:3], sg.at[0:3], ssend.at[1], srecv.at[1], sib).wait_recv()

    def project(xs):
        start = pl.multiple_of(xs * ROWS, 16)
        n = ROWS

        def pair(jj, _):
            t = tok[xs]
            up = jnp.dot(
                t, wb[:, pl.ds(pl.multiple_of(jj * 256, 256), 256)], preferred_element_type=f32
            )
            gate = jnp.dot(
                t,
                wb[:, pl.ds(pl.multiple_of(512 + jj * 256, 256), 256)],
                preferred_element_type=f32,
            )
            for i in range(2):
                j = 2 * jj + i
                u = up[:, i * GD:(i + 1) * GD].astype(bf16).astype(f32)
                op[j, pl.ds(start, n), :] = gelu(u)
                a = gelu(gate[:, i * GD:(i + 1) * GD].astype(bf16).astype(f32))
                a = a - jnp.mean(a, axis=-1, keepdims=True)
                spread = jnp.mean(a * a, axis=-1, keepdims=True)
                v[j, pl.ds(start, n), :] = (
                    a * lax.rsqrt(spread + norm_eps) * sg[j]
                ).astype(bf16)
            return 0

        lax.fori_loop(0, 2, pair, 0)

    def spread_bias(j, _):
        bt[j] = jnp.transpose(jnp.broadcast_to(sb[j], (GD, SPAN)))
        return 0

    project(x)
    yrun(ystep, (5, 6), (2,))
    yrun(ystep, (7,), (0, 1))
    for k in range(XN):
        slot = xslot(mod(x + 1 + 2 * c, NX), k)
        remote(slot, slot, xsend.at[0], xrecv.at[(1 - c) * XN + k], sib).wait_recv()
    project(xfrom1)
    yrun(ystep, (7,), (2,))
    yrun(pystep, (0,), (0, 1))
    qpair(1)
    project(mod(x + 1 + 2 * c, NX))
    yrun(pystep, (0,), (2,))
    yrun(pystep, (1, 2), (0, 1))
    ppair(2)
    lax.fori_loop(0, 4, spread_bias, 0)
    for k in range(XN):
        slot = xslot(xfrom2, k)
        remote(slot, slot, xsend.at[0], xrecv.at[2 * XN + k], sib).wait_recv()
    project(xfrom2)
    yrun(pystep, (1, 2), (2,))
    yrun(pystep, (3, 4), (0, 1))
    qpair(2)

    for cc in range(2):
        @pl.when(c != cc)
        def _():
            wait_all(mb.at[:, 0:MSUM[cc], :], 0)

    kmax = (384, 640, 1024, 1280)
    kfree = (0, 256, 640, 896)

    def lanes(j, xx):
        return pl.ds(pl.multiple_of((4 * j + xx) * GD, GD), GD)

    def acopy(j, r):
        src = g.at[j, pl.ds(ROWS * r, ROWS), :]
        return remote(src, ab.at[:, lanes(j, x)], asend.at[0], arecv.at[j], dev(r, y, z, c))

    def alocal(j, r):
        src = g.at[j, pl.ds(ROWS * r, ROWS), :]
        return pltpu.make_async_copy(src, ab.at[:, lanes(j, x)], asem.at[0])

    def mix(j, _):
        for r in range(4):
            rows = pl.ds(ROWS * r, ROWS)
            k0, k1 = kfree[r], kmax[r]
            at_row = lax.broadcasted_iota(jnp.int32, (ROWS, k1 - k0), 0) + ROWS * r
            at_col = lax.broadcasted_iota(jnp.int32, (ROWS, k1 - k0), 1) + k0
            edge = mb[j, rows, k0:k1].astype(f32)
            edge = jnp.where(at_col <= at_row, edge, 0.0).astype(bf16)
            total = jnp.dot(edge, v[j, k0:k1, :], preferred_element_type=f32)
            if k0:
                total += jnp.dot(
                    mb[j, rows, 0:k0], v[j, 0:k0, :], preferred_element_type=f32
                )
            g[j, rows, :] = (op[j, rows, :] * (total + bt[j, rows, :])).astype(bf16)

        for r in range(4):
            @pl.when(x != r)
            def _():
                acopy(j, r).start()

            @pl.when(x == r)
            def _():
                alocal(j, r).start()
        return 0

    lax.fori_loop(0, 2, mix, 0)
    ppair(3)
    lax.fori_loop(2, 4, mix, 0)
    yrun(pystep, (3, 4), (2,))
    yrun(pystep, (5, 6), (0, 1))
    qpair(3)
    pstep(4)
    yrun(pystep, (5, 6), (2,))
    yrun(pystep, (7,), (0, 1))
    qstep(4, 0)
    qstep(4, 1)
    yrun(pystep, (7,), (2,))

    for j in range(4):
        slot = ab.at[:, 0:3 * GD]
        remote(slot, slot, asend.at[0], arecv.at[j], sib).wait_recv()
    pltpu.make_async_copy(ab.at[:, 0:4 * GD], ab.at[:, 0:4 * GD], asem.at[0]).wait()

    def rms(i, _):
        rows = pl.ds(pl.multiple_of(i * 64, 16), 64)
        a = ab[rows, :].astype(f32)
        scale = lax.rsqrt(jnp.mean(a * a, axis=-1, keepdims=True) + norm_eps)
        nb[rows, :] = (a * scale * ogain[...]).astype(bf16)
        return 0

    lax.fori_loop(0, ROWS // 64, rms, 0)
    wait_all(ob.at[0:OZ, 0:1024], 2)
    wait_all(ob.at[0:WIDTH - OZ, 0:1024], 3)

    def emit(i, _):
        cols = pl.ds(pl.multiple_of(i * 1024, 1024), 1024)
        out_ref[0, :, cols] = jnp.dot(nb[...], ob[:, cols], preferred_element_type=f32).astype(bf16)
        return 0

    lax.fori_loop(0, 2, emit, 0)

    def sent(ref, sem):
        remote(ref, ref, sem, brecv.at[0], sib).wait_send()

    sent(sb.at[0:3], ssend.at[0])
    sent(sg.at[0:3], ssend.at[1])
    sent(tok.at[0:3], xsend.at[0])
    sent(wb.at[0:896, :], zwsend.at[0])
    sent(ob.at[0:OZ, 0:896], zqsend.at[0])
    sent(ob.at[0:OQ, 0:896], zpsend.at[0])
    sent(ob.at[0:OQ * 2, 0:1536], oysend.at[0])
    sent(wb.at[0:1024, :], bsend.at[1])
    sent(ob.at[0:OZ, 0:1024], bsend.at[2])
    sent(ob.at[0:WIDTH - OZ, 0:1024], bsend.at[3])
    sent(ab.at[:, 0:12 * GD], asend.at[0])
    for cc in range(2):
        @pl.when(c == cc)
        def _():
            sent(mb.at[:, 0:MSUM[cc], :], bsend.at[0])
            sent(mb.at[0:3, 0:MSUM[cc], :], ysend.at[0])

    def msent(i, _):
        r, w = lax.div(i, 2), lax.rem(i, 2)
        org = mod(z + lax.select(w == 0, NZ - r, r), NZ)

        def go(width):
            slot = mslot(y, org * 2 + c, width)
            remote(slot, slot, zmsend.at[i], zmrecv.at[0], sib).wait_send()

        @pl.when((i < 6) | (w == c))
        def _():
            by_width(org * 2 + c, go)
        return 0

    lax.fori_loop(0, 8, msent, 0)


def body(tokens, up_weight, gate_weight, group_gain, mix_weight, mix_bias, out_gain, out_weight):
    hbm = pl.BlockSpec(memory_space=pl.ANY)
    vmem = pl.BlockSpec(memory_space=pltpu.VMEM)
    dma = pltpu.SemaphoreType.DMA
    return pl.pallas_call(
        kernel,
        out_shape=jax.ShapeDtypeStruct((1, ROWS, WIDTH), bf16),
        in_specs=[hbm, hbm, hbm, hbm, hbm, hbm, vmem, hbm],
        out_specs=vmem,
        scratch_shapes=[
            pltpu.VMEM((NX, ROWS, WIDTH), bf16),
            pltpu.VMEM((WIDTH, 1024), bf16),
            pltpu.VMEM((4, SPAN, SPAN), bf16),
            pltpu.VMEM((WIDTH, WIDTH), bf16),
            pltpu.VMEM((4, SPAN, GD), bf16),
            pltpu.VMEM((4, SPAN, GD), f32),
            pltpu.VMEM((4, SPAN, GD), f32),
            pltpu.VMEM((4, SPAN, GD), bf16),
            pltpu.VMEM((ROWS, WIDTH), bf16),
            pltpu.VMEM((ROWS, WIDTH), bf16),
            pltpu.VMEM((4, 1, SPAN), f32),
            pltpu.VMEM((4, 1, GD), f32),
            dma((6,)),
            dma((1,)),
            dma((12,)),
            dma((8,)),
            dma((8,)),
            dma((1,)),
            dma((16,)),
            dma((1,)),
            dma((16,)),
            dma((1,)),
            dma((8,)),
            dma((1,)),
            dma((24,)),
            dma((1,)),
            dma((24,)),
            dma((4,)),
            dma((4,)),
            dma((1,)),
            dma((4,)),
            dma((2,)),
            dma((2,)),
            dma((1,)),
        ],
        compiler_params=pltpu.CompilerParams(
            collective_id=0, has_side_effects=True, vmem_limit_bytes=66_000_000
        ),
        name="gating",
    )(
        tokens, up_weight, gate_weight, group_gain, mix_weight, mix_bias,
        out_gain.reshape(1, WIDTH), out_weight,
    )


def solution(mesh):
    return jax.shard_map(
        body,
        mesh=mesh,
        in_specs=(
            P("dp", "sp", None),
            P("dp", None),
            P("dp", None),
            P("sp", None),
            P("sp", "dp", None),
            P("sp", None),
            P(),
            P(None, "dp"),
        ),
        out_specs=P("dp", "sp", None),
        check_vma=False,
    )
```

```python
import functools

import jax
import jax.numpy as jnp
from jax import lax
from jax.experimental import pallas as pl
from jax.experimental.pallas import tpu as pltpu
from jax.sharding import PartitionSpec as P

norm_eps = 1e-06
NX, NY, NZ = 4, 4, 8
ROWS = 320
SPAN = 1280
WIDTH = 2048
GD = 128
MROWS = 80
OZ = 1024
OQ = (WIDTH - OZ) // 4
XN = 4
XR = ROWS // XN
MSUM = (352, 384)
f32 = jnp.float32
bf16 = jnp.bfloat16


def remote(src, dst, send, recv, dev):
    return pltpu.make_async_remote_copy(
        src_ref=src,
        dst_ref=dst,
        send_sem=send,
        recv_sem=recv,
        device_id=dev,
        device_id_type=pl.DeviceIdType.MESH,
    )


def gelu(a):
    return 0.5 * a * (1.0 + jnp.tanh(0.7978845608028654 * (a + 0.044715 * (a * a * a))))


def kernel(
    tokens, upw, gatew, gain, mixw, bias, ogain, outw, out_ref,
    tok, wb, mb, ob, v, op, bt, g, ab, nb, sb, sg,
    lsem, xsend, xrecv, zmsend, zmrecv, zwsend, zwrecv, zqsend, zqrecv,
    zpsend, zprecv, ysend, yrecv, oysend, oyrecv, bsend, brecv,
    asend, arecv, ssend, srecv, asem, osem, ov, og,
):
    sp = lax.axis_index("sp")
    dp = lax.axis_index("dp")
    y, x = lax.div(sp, NX), lax.rem(sp, NX)
    z, c = lax.div(dp, 2), lax.rem(dp, 2)

    def dev(xx, yy, zz, cc):
        return {"sp": yy * NX + xx, "dp": zz * 2 + cc}

    def mod(a, n):
        return lax.rem(a, n)

    tox = [dev(mod(x + 1, NX), y, z, c), dev(mod(x + NX - 1, NX), y, z, c)]
    toy = [dev(x, mod(y + 1, NY), z, c), dev(x, mod(y + NY - 1, NY), z, c)]
    toz = [dev(x, y, mod(z + 1, NZ), c), dev(x, y, mod(z + NZ - 1, NZ), c)]
    sib = dev(x, y, z, 1 - c)

    def xorg(r, way):
        return mod(x + (NX - r if way == 0 else r), NX)

    def yorg(r, way):
        return mod(y + (NY - r if way == 0 else r), NY)

    def zorg(r, way):
        return mod(z + (NZ - r if way == 0 else r), NZ)

    d = z * 2 + c
    wrow = pl.ds(pl.multiple_of(d * GD, GD), GD)
    loads = [
        pltpu.make_async_copy(
            mixw.at[0], mb.at[y, pl.ds(pl.multiple_of(d * MROWS, 16), MROWS), :], lsem.at[1]
        ),
        pltpu.make_async_copy(tokens.at[0], tok.at[x], lsem.at[0]),
        pltpu.make_async_copy(outw, ob.at[:, wrow], lsem.at[2]),
        pltpu.make_async_copy(bias, sb.at[y], lsem.at[3]),
        pltpu.make_async_copy(gain, sg.at[y], lsem.at[4]),
        pltpu.make_async_copy(ogain, og, lsem.at[6]),
    ]
    for load in loads:
        load.start()
    for j in range(4):
        cols = pl.ds(pl.multiple_of((x + 4 * j) * GD, GD), GD)
        for half, w in enumerate((upw, gatew)):
            pltpu.make_async_copy(
                w.at[:, cols], wb.at[wrow, pl.ds(512 * half + j * GD, GD)], lsem.at[5]
            ).start()
    loads.append(pltpu.make_async_copy(wb.at[wrow, :], wb.at[wrow, :], lsem.at[5]))

    barrier = pltpu.get_barrier_semaphore()
    peers = [dev(mod(x + k, NX), y, z, c) for k in (1, 2, 3)]
    peers += [dev(x, mod(y + k, NY), z, c) for k in (1, 2, 3)]
    peers += toz + [sib]
    for peer in peers:
        pl.semaphore_signal(barrier, inc=1, device_id=peer, device_id_type=pl.DeviceIdType.MESH)
    pl.semaphore_wait(barrier, len(peers))
    for load in loads:
        load.wait()

    def xslot(shard, k):
        return tok.at[shard, pl.ds(k * XR, XR), :]

    xfrom1 = mod(x + NX - 1 + 2 * c, NX)
    xfrom2 = mod(x + 2, NX)
    xto = dev(mod(x + 1 + 2 * c, NX), y, z, c)

    def xforward(k):
        slot = xslot(xfrom1, k)
        remote(slot, slot, xsend.at[0], xrecv.at[c * XN + k], xto).wait_recv()
        remote(slot, slot, xsend.at[0], xrecv.at[2 * XN + k], xto).start()

    def by_width(dd, fn):
        n = lax.div(MROWS * (dd + 1) + GD - 1, GD)
        for k in range(1, 11):
            @pl.when(n == k)
            def _():
                fn(GD * k)

    def mslot(group, dd, width):
        return mb.at[group, pl.ds(pl.multiple_of(dd * MROWS, 16), MROWS), pl.ds(0, width)]

    def steps(r, way):
        if r == 0:
            return z, None, [0, 1], 0
        if r == 4:
            return mod(z + 4, NZ), 6 + c, [], 7
        return zorg(r, way), (r - 1) * 2 + way, [way], 2 * r - 1 + way

    def onward(r, way, start):
        for w in way:
            if r < 3:
                start(w)
            else:
                @pl.when(c == w)
                def _():
                    start(w)

    def mstep(r, way=None):
        org, at, ways, k = steps(r, way)
        dd = org * 2 + c

        def go(width):
            slot = mslot(y, dd, width)
            if at is not None:
                remote(slot, slot, zmsend.at[0], zmrecv.at[at], sib).wait_recv()

            def start(w):
                i = r * 2 + w
                remote(slot, slot, zmsend.at[i], zmrecv.at[i], toz[w]).start()

            onward(r, ways, start)
            for w in range(2):
                remote(slot, slot, ysend.at[0], yrecv.at[w * 8 + k], toy[w]).start()
            remote(slot, slot, bsend.at[0], brecv.at[0], sib).start()

        by_width(dd, go)

    def ygroup(a):
        return mod(y + 2, NY) if a == 2 else yorg(1, a)

    def kchip(k):
        if k == 0:
            return z
        if k == 7:
            return mod(z + 4, NZ)
        return zorg((k + 1) // 2, (k + 1) % 2)

    def ystep(a, k):
        dd = kchip(k) * 2 + c

        def go(width):
            slot = mslot(ygroup(a), dd, width)
            remote(slot, slot, ysend.at[0], yrecv.at[a * 8 + k], sib).wait_recv()
            if a < 2:
                @pl.when(c == a)
                def _():
                    remote(slot, slot, ysend.at[0], yrecv.at[16 + k], toy[a]).start()
            remote(slot, slot, bsend.at[0], brecv.at[0], sib).start()

        by_width(dd, go)

    def wstep(r, half, way=None):
        org, at, ways, k = steps(r, way)
        slot = wb.at[
            pl.ds(pl.multiple_of((org * 2 + c) * GD, GD), GD), pl.ds(512 * half, 512)
        ]
        if at is not None:
            remote(slot, slot, zwsend.at[0], zwrecv.at[at * 2 + half], sib).wait_recv()

        def start(w):
            i = (r * 2 + w) * 2 + half
            remote(slot, slot, zwsend.at[0], zwrecv.at[i], toz[w]).start()

        onward(r, ways, start)
        remote(slot, slot, bsend.at[1], brecv.at[1], sib).start()

    def qstep(r, half, way=None):
        org, at, ways, k = steps(r, way)
        slot = ob.at[
            pl.ds(OZ // 2 * half, OZ // 2), pl.ds(pl.multiple_of((org * 2 + c) * GD, GD), GD)
        ]
        if at is not None:
            remote(slot, slot, zqsend.at[0], zqrecv.at[at * 2 + half], sib).wait_recv()

        def start(w):
            i = (r * 2 + w) * 2 + half
            remote(slot, slot, zqsend.at[0], zqrecv.at[i], toz[w]).start()

        onward(r, ways, start)
        remote(slot, slot, bsend.at[2], brecv.at[2], sib).start()

    def pslot(group, chip):
        rows = pl.ds(pl.multiple_of(OZ + OQ * group, 16), OQ)
        return ob.at[rows, pl.ds(pl.multiple_of((chip * 2 + c) * GD, GD), GD)]

    def pstep(r, way=None):
        org, at, ways, k = steps(r, way)
        slot = pslot(y, org)
        if at is not None:
            remote(slot, slot, zpsend.at[0], zprecv.at[at], sib).wait_recv()

        def start(w):
            i = r * 2 + w
            remote(slot, slot, zpsend.at[0], zprecv.at[i], toz[w]).start()

        onward(r, ways, start)
        for w in range(2):
            remote(slot, slot, oysend.at[0], oyrecv.at[w * 8 + k], toy[w]).start()
        remote(slot, slot, bsend.at[3], brecv.at[3], sib).start()

    def pystep(a, k):
        slot = pslot(ygroup(a), kchip(k))
        remote(slot, slot, oysend.at[0], oyrecv.at[a * 8 + k], sib).wait_recv()
        if a < 2:
            @pl.when(c == a)
            def _():
                remote(slot, slot, oysend.at[0], oyrecv.at[16 + k], toy[a]).start()
        remote(slot, slot, bsend.at[3], brecv.at[3], sib).start()

    def yrun(fn, ks, ways):
        for k in ks:
            for a in ways:
                fn(a, k)

    def mpair(r):
        mstep(r, 0)
        mstep(r, 1)

    def wpair(r):
        for half in range(2):
            wstep(r, half, 0)
            wstep(r, half, 1)

    def qpair(r):
        for half in range(2):
            qstep(r, half, 0)
            qstep(r, half, 1)

    def ppair(r):
        pstep(r, 0)
        pstep(r, 1)

    mstep(0)
    for k in range(XN):
        for w in range(2):
            remote(xslot(x, k), xslot(x, k), xsend.at[0], xrecv.at[w * XN + k], tox[w]).start()
    wstep(0, 0)
    wstep(0, 1)
    for k in (1, 2, 3):
        peer = dev(x, mod(y + k, NY), z, c)
        remote(sb.at[y], sb.at[y], ssend.at[0], srecv.at[0], peer).start()
        remote(sg.at[y], sg.at[y], ssend.at[1], srecv.at[1], peer).start()

    mpair(1)
    yrun(ystep, (0,), (0, 1))
    wpair(1)
    mpair(2)
    yrun(ystep, (1, 2), (0, 1))
    xforward(0)
    wpair(2)
    yrun(ystep, (0,), (2,))
    mpair(3)
    xforward(1)
    yrun(ystep, (3, 4), (0, 1))
    wpair(3)
    pstep(0)
    qstep(0, 0)
    qstep(0, 1)
    mstep(4)
    xforward(2)
    yrun(ystep, (5, 6), (0, 1))
    yrun(ystep, (1, 2), (2,))
    wstep(4, 0)
    wstep(4, 1)
    xforward(3)
    yrun(ystep, (7,), (0, 1))
    ppair(1)

    def wait_all(ref, i):
        remote(ref, ref, bsend.at[i], brecv.at[i], sib).wait_recv()

    wait_all(wb.at[0:1024, :], 1)
    remote(sb.at[0:3], sb.at[0:3], ssend.at[0], srecv.at[0], sib).wait_recv()
    remote(sg.at[0:3], sg.at[0:3], ssend.at[1], srecv.at[1], sib).wait_recv()

    def project(xs):
        start = pl.multiple_of(xs * ROWS, 16)
        n = ROWS

        def pair(jj, _):
            t = tok[xs]
            up = jnp.dot(
                t, wb[:, pl.ds(pl.multiple_of(jj * 256, 256), 256)], preferred_element_type=f32
            )
            gate = jnp.dot(
                t,
                wb[:, pl.ds(pl.multiple_of(512 + jj * 256, 256), 256)],
                preferred_element_type=f32,
            )
            for i in range(2):
                j = 2 * jj + i
                u = up[:, i * GD:(i + 1) * GD].astype(bf16).astype(f32)
                op[j, pl.ds(start, n), :] = gelu(u)
                a = gelu(gate[:, i * GD:(i + 1) * GD].astype(bf16).astype(f32))
                a = a - jnp.mean(a, axis=-1, keepdims=True)
                spread = jnp.mean(a * a, axis=-1, keepdims=True)
                v[j, pl.ds(start, n), :] = (
                    a * lax.rsqrt(spread + norm_eps) * sg[j]
                ).astype(bf16)
            return 0

        lax.fori_loop(0, 2, pair, 0)

    def spread_bias(j, _):
        bt[j] = jnp.transpose(jnp.broadcast_to(sb[j], (GD, SPAN)))
        return 0

    project(x)
    yrun(pystep, (0,), (0, 1))
    yrun(ystep, (3, 4), (2,))
    for k in range(XN):
        slot = xslot(mod(x + 1 + 2 * c, NX), k)
        remote(slot, slot, xsend.at[0], xrecv.at[(1 - c) * XN + k], sib).wait_recv()
    project(xfrom1)
    qpair(1)
    yrun(ystep, (5, 6), (2,))
    project(mod(x + 1 + 2 * c, NX))
    ppair(2)
    yrun(pystep, (1, 2), (0, 1))
    lax.fori_loop(0, 4, spread_bias, 0)
    yrun(ystep, (7,), (2,))
    for k in range(XN):
        slot = xslot(xfrom2, k)
        remote(slot, slot, xsend.at[0], xrecv.at[2 * XN + k], sib).wait_recv()
    project(xfrom2)
    yrun(pystep, (0,), (2,))

    for cc in range(2):
        @pl.when(c != cc)
        def _():
            wait_all(mb.at[:, 0:MSUM[cc], :], 0)

    kmax = (384, 640, 1024, 1280)
    kfree = (0, 256, 640, 896)

    def lanes(j, xx):
        return pl.ds(pl.multiple_of((4 * j + xx) * GD, GD), GD)

    def acopy(j, r):
        src = g.at[j, pl.ds(ROWS * r, ROWS), :]
        return remote(src, ab.at[:, lanes(j, x)], asend.at[0], arecv.at[j], dev(r, y, z, c))

    def alocal(j, r):
        src = g.at[j, pl.ds(ROWS * r, ROWS), :]
        return pltpu.make_async_copy(src, ab.at[:, lanes(j, x)], asem.at[0])

    def mix(j, _):
        for r in range(4):
            rows = pl.ds(ROWS * r, ROWS)
            k0, k1 = kfree[r], kmax[r]
            at_row = lax.broadcasted_iota(jnp.int32, (ROWS, k1 - k0), 0) + ROWS * r
            at_col = lax.broadcasted_iota(jnp.int32, (ROWS, k1 - k0), 1) + k0
            edge = mb[j, rows, k0:k1].astype(f32)
            edge = jnp.where(at_col <= at_row, edge, 0.0).astype(bf16)
            total = jnp.dot(edge, v[j, k0:k1, :], preferred_element_type=f32)
            if k0:
                total += jnp.dot(
                    mb[j, rows, 0:k0], v[j, 0:k0, :], preferred_element_type=f32
                )
            g[j, rows, :] = (op[j, rows, :] * (total + bt[j, rows, :])).astype(bf16)

        for r in range(4):
            @pl.when(x != r)
            def _():
                acopy(j, r).start()

            @pl.when(x == r)
            def _():
                alocal(j, r).start()
        return 0

    lax.fori_loop(0, 2, mix, 0)
    yrun(pystep, (3, 4), (0, 1))
    lax.fori_loop(2, 4, mix, 0)
    ppair(3)
    qpair(2)
    yrun(pystep, (1, 2), (2,))
    yrun(pystep, (3, 4), (2,))
    pstep(4)
    qstep(3, 0, 0)
    qstep(3, 0, 1)
    yrun(pystep, (5, 6), (0, 1))
    qstep(3, 1, 0)
    qstep(3, 1, 1)
    yrun(pystep, (7,), (0, 1))
    yrun(pystep, (5, 6), (2,))
    qstep(4, 0)
    yrun(pystep, (7,), (2,))
    qstep(4, 1)

    for j in range(4):
        slot = ab.at[:, 0:3 * GD]
        remote(slot, slot, asend.at[0], arecv.at[j], sib).wait_recv()
    pltpu.make_async_copy(ab.at[:, 0:4 * GD], ab.at[:, 0:4 * GD], asem.at[0]).wait()

    def rms(i, _):
        rows = pl.ds(pl.multiple_of(i * 64, 16), 64)
        a = ab[rows, :].astype(f32)
        scale = lax.rsqrt(jnp.mean(a * a, axis=-1, keepdims=True) + norm_eps)
        nb[rows, :] = (a * scale * og[...]).astype(bf16)
        return 0

    lax.fori_loop(0, ROWS // 64, rms, 0)
    wait_all(ob.at[0:OZ, 0:1024], 2)
    wait_all(ob.at[0:WIDTH - OZ, 0:1024], 3)

    def emit(i, _):
        cols = pl.ds(pl.multiple_of(i * 1024, 1024), 1024)
        ov[:, cols] = jnp.dot(nb[...], ob[:, cols], preferred_element_type=f32).astype(bf16)
        pltpu.make_async_copy(ov.at[:, cols], out_ref.at[0, :, cols], osem.at[0]).start()
        return 0

    lax.fori_loop(0, 2, emit, 0)

    def sent(ref, sem):
        remote(ref, ref, sem, brecv.at[0], sib).wait_send()

    sent(sb.at[0:3], ssend.at[0])
    sent(sg.at[0:3], ssend.at[1])
    sent(tok.at[0:3], xsend.at[0])
    sent(wb.at[0:896, :], zwsend.at[0])
    sent(ob.at[0:OZ, 0:896], zqsend.at[0])
    sent(ob.at[0:OQ, 0:896], zpsend.at[0])
    sent(ob.at[0:OQ * 2, 0:1536], oysend.at[0])
    sent(wb.at[0:1024, :], bsend.at[1])
    sent(ob.at[0:OZ, 0:1024], bsend.at[2])
    sent(ob.at[0:WIDTH - OZ, 0:1024], bsend.at[3])
    sent(ab.at[:, 0:12 * GD], asend.at[0])
    for cc in range(2):
        @pl.when(c == cc)
        def _():
            sent(mb.at[:, 0:MSUM[cc], :], bsend.at[0])
            sent(mb.at[0:3, 0:MSUM[cc], :], ysend.at[0])

    def msent(i, _):
        r, w = lax.div(i, 2), lax.rem(i, 2)
        org = mod(z + lax.select(w == 0, NZ - r, r), NZ)

        def go(width):
            slot = mslot(y, org * 2 + c, width)
            remote(slot, slot, zmsend.at[i], zmrecv.at[0], sib).wait_send()

        @pl.when((i < 6) | (w == c))
        def _():
            by_width(org * 2 + c, go)
        return 0

    lax.fori_loop(0, 8, msent, 0)
    pltpu.make_async_copy(ov, out_ref.at[0], osem.at[0]).wait()


def body(tokens, up_weight, gate_weight, group_gain, mix_weight, mix_bias, out_gain, out_weight):
    hbm = pl.BlockSpec(memory_space=pltpu.HBM)
    dma = pltpu.SemaphoreType.DMA
    return pl.pallas_call(
        kernel,
        out_shape=jax.ShapeDtypeStruct((1, ROWS, WIDTH), bf16),
        in_specs=[hbm] * 8,
        out_specs=pl.BlockSpec(memory_space=pl.ANY),
        scratch_shapes=[
            pltpu.VMEM((NX, ROWS, WIDTH), bf16),
            pltpu.VMEM((WIDTH, 1024), bf16),
            pltpu.VMEM((4, SPAN, SPAN), bf16),
            pltpu.VMEM((WIDTH, WIDTH), bf16),
            pltpu.VMEM((4, SPAN, GD), bf16),
            pltpu.VMEM((4, SPAN, GD), f32),
            pltpu.VMEM((4, SPAN, GD), f32),
            pltpu.VMEM((4, SPAN, GD), bf16),
            pltpu.VMEM((ROWS, WIDTH), bf16),
            pltpu.VMEM((ROWS, WIDTH), bf16),
            pltpu.VMEM((4, 1, SPAN), f32),
            pltpu.VMEM((4, 1, GD), f32),
            dma((7,)),
            dma((1,)),
            dma((12,)),
            dma((8,)),
            dma((8,)),
            dma((1,)),
            dma((16,)),
            dma((1,)),
            dma((16,)),
            dma((1,)),
            dma((8,)),
            dma((1,)),
            dma((24,)),
            dma((1,)),
            dma((24,)),
            dma((4,)),
            dma((4,)),
            dma((1,)),
            dma((4,)),
            dma((2,)),
            dma((2,)),
            dma((1,)),
            dma((1,)),
            pltpu.VMEM((ROWS, WIDTH), bf16),
            pltpu.VMEM((1, WIDTH), f32),
        ],
        compiler_params=pltpu.CompilerParams(
            collective_id=0, has_side_effects=True, vmem_limit_bytes=46_000_000
        ),
        name="gating",
    )(
        *(
            pltpu.with_memory_space_constraint(a, pltpu.HBM)
            for a in (
                tokens, up_weight, gate_weight, group_gain, mix_weight, mix_bias,
                out_gain.reshape(1, WIDTH), out_weight,
            )
        )
    )


def solution(mesh):
    return jax.shard_map(
        body,
        mesh=mesh,
        in_specs=(
            P("dp", "sp", None),
            P("dp", None),
            P("dp", None),
            P("sp", None),
            P("sp", "dp", None),
            P("sp", None),
            P(),
            P(None, "dp"),
        ),
        out_specs=P("dp", "sp", None),
        check_vma=False,
    )
```

```python
import functools

import jax
import jax.numpy as jnp
from jax import lax
from jax.experimental import pallas as pl
from jax.experimental.pallas import tpu as pltpu
from jax.sharding import PartitionSpec as P

norm_eps = 1e-06
NX, NY, NZ = 4, 4, 8
ROWS = 320
SPAN = 1280
WIDTH = 2048
GD = 128
MROWS = 80
OZ = 768
OQ = (WIDTH - OZ) // 4
XN = 4
XR = ROWS // XN
MSUM = (352, 384)
f32 = jnp.float32
bf16 = jnp.bfloat16


def remote(src, dst, send, recv, dev):
    return pltpu.make_async_remote_copy(
        src_ref=src,
        dst_ref=dst,
        send_sem=send,
        recv_sem=recv,
        device_id=dev,
        device_id_type=pl.DeviceIdType.MESH,
    )


def gelu(a):
    return 0.5 * a * (1.0 + jnp.tanh(0.7978845608028654 * (a + 0.044715 * (a * a * a))))


def kernel(
    tokens, upw, gatew, gain, mixw, bias, ogain, outw, out_ref,
    tok, wb, mb, ob, v, op, bt, g, ab, nb, sb, sg,
    lsem, xsend, xrecv, zmsend, zmrecv, zwsend, zwrecv, zqsend, zqrecv,
    zpsend, zprecv, ysend, yrecv, oysend, oyrecv, bsend, brecv,
    asend, arecv, ssend, srecv, asem, osem, ov, og, acc, ss, pa,
):
    sp = lax.axis_index("sp")
    dp = lax.axis_index("dp")
    y, x = lax.div(sp, NX), lax.rem(sp, NX)
    z, c = lax.div(dp, 2), lax.rem(dp, 2)

    def dev(xx, yy, zz, cc):
        return {"sp": yy * NX + xx, "dp": zz * 2 + cc}

    def mod(a, n):
        return lax.rem(a, n)

    tox = [dev(mod(x + 1, NX), y, z, c), dev(mod(x + NX - 1, NX), y, z, c)]
    toy = [dev(x, mod(y + 1, NY), z, c), dev(x, mod(y + NY - 1, NY), z, c)]
    toz = [dev(x, y, mod(z + 1, NZ), c), dev(x, y, mod(z + NZ - 1, NZ), c)]
    sib = dev(x, y, z, 1 - c)

    def xorg(r, way):
        return mod(x + (NX - r if way == 0 else r), NX)

    def yorg(r, way):
        return mod(y + (NY - r if way == 0 else r), NY)

    def zorg(r, way):
        return mod(z + (NZ - r if way == 0 else r), NZ)

    d = z * 2 + c
    wrow = pl.ds(pl.multiple_of(d * GD, GD), GD)
    loads = [
        pltpu.make_async_copy(
            mixw.at[0], mb.at[y, pl.ds(pl.multiple_of(d * MROWS, 16), MROWS), :], lsem.at[1]
        ),
        pltpu.make_async_copy(tokens.at[0], tok.at[x], lsem.at[0]),
        pltpu.make_async_copy(outw, ob.at[:, wrow], lsem.at[2]),
        pltpu.make_async_copy(bias, sb.at[y], lsem.at[3]),
        pltpu.make_async_copy(gain, sg.at[y], lsem.at[4]),
        pltpu.make_async_copy(ogain, og, lsem.at[6]),
    ]
    for load in loads:
        load.start()
    for j in range(4):
        cols = pl.ds(pl.multiple_of((x + 4 * j) * GD, GD), GD)
        for half, w in enumerate((upw, gatew)):
            pltpu.make_async_copy(
                w.at[:, cols], wb.at[wrow, pl.ds(512 * half + j * GD, GD)], lsem.at[5]
            ).start()
    loads.append(pltpu.make_async_copy(wb.at[wrow, :], wb.at[wrow, :], lsem.at[5]))

    barrier = pltpu.get_barrier_semaphore()
    peers = [dev(mod(x + k, NX), y, z, c) for k in (1, 2, 3)]
    peers += [dev(x, mod(y + k, NY), z, c) for k in (1, 2, 3)]
    peers += toz + [sib]
    for peer in peers:
        pl.semaphore_signal(barrier, inc=1, device_id=peer, device_id_type=pl.DeviceIdType.MESH)
    pl.semaphore_wait(barrier, len(peers))
    for load in loads:
        load.wait()

    def xslot(shard, k):
        return tok.at[shard, pl.ds(k * XR, XR), :]

    xfrom1 = mod(x + NX - 1 + 2 * c, NX)
    xfrom2 = mod(x + 2, NX)
    xto = dev(mod(x + 1 + 2 * c, NX), y, z, c)

    def xforward(k):
        slot = xslot(xfrom1, k)
        remote(slot, slot, xsend.at[0], xrecv.at[c * XN + k], xto).wait_recv()
        remote(slot, slot, xsend.at[0], xrecv.at[2 * XN + k], xto).start()

    def by_width(dd, fn):
        n = lax.div(MROWS * (dd + 1) + GD - 1, GD)
        for k in range(1, 11):
            @pl.when(n == k)
            def _():
                fn(GD * k)

    def mslot(group, dd, width):
        return mb.at[group, pl.ds(pl.multiple_of(dd * MROWS, 16), MROWS), pl.ds(0, width)]

    def last_way(chip):
        return lax.div(mod(chip + 6, NZ), 4)

    light = [last_way(mod(z + 1, NZ)) == 0, last_way(mod(z + NZ - 1, NZ)) == 1]
    alternate = [c == 0, c == 1]

    def steps(r, way):
        if r == 0:
            return z, None, [0, 1], 0
        if r == 4:
            return mod(z + 4, NZ), 6, [], 7
        return zorg(r, way), (r - 1) * 2 + way, [way], 2 * r - 1 + way

    def onward(r, way, start, last):
        for w in way:
            if r < 3:
                start(w)
            else:
                @pl.when(last[w])
                def _():
                    start(w)

    def mstep(r, way=None):
        org, at, ways, k = steps(r, way)
        if r == 4:
            at = at + last_way(z)
        dd = org * 2 + c

        def go(width):
            slot = mslot(y, dd, width)
            if at is not None:
                remote(slot, slot, zmsend.at[0], zmrecv.at[at], sib).wait_recv()

            def start(w):
                i = r * 2 + w
                remote(slot, slot, zmsend.at[i], zmrecv.at[i], toz[w]).start()

            onward(r, ways, start, light)
            for w in range(2):
                remote(slot, slot, ysend.at[0], yrecv.at[w * 8 + k], toy[w]).start()
            remote(slot, slot, bsend.at[0], brecv.at[0], sib).start()

        by_width(dd, go)

    def ygroup(a):
        return mod(y + 2, NY) if a == 2 else yorg(1, a)

    def kchip(k):
        if k == 0:
            return z
        if k == 7:
            return mod(z + 4, NZ)
        return zorg((k + 1) // 2, (k + 1) % 2)

    def ystep(a, k):
        dd = kchip(k) * 2 + c

        def go(width):
            slot = mslot(ygroup(a), dd, width)
            remote(slot, slot, ysend.at[0], yrecv.at[a * 8 + k], sib).wait_recv()
            if a < 2:
                @pl.when(c == a)
                def _():
                    remote(slot, slot, ysend.at[0], yrecv.at[16 + k], toy[a]).start()
            remote(slot, slot, bsend.at[0], brecv.at[0], sib).start()

        by_width(dd, go)

    def wstep(r, half, way=None):
        org, at, ways, k = steps(r, way)
        if r == 4:
            at = at + last_way(z)
        slot = wb.at[
            pl.ds(pl.multiple_of((org * 2 + c) * GD, GD), GD), pl.ds(512 * half, 512)
        ]
        if at is not None:
            remote(slot, slot, zwsend.at[0], zwrecv.at[at * 2 + half], sib).wait_recv()

        def start(w):
            i = (r * 2 + w) * 2 + half
            remote(slot, slot, zwsend.at[0 if r < 3 else 1 + w], zwrecv.at[i], toz[w]).start()

        onward(r, ways, start, light)
        remote(slot, slot, bsend.at[1], brecv.at[1 if r < 3 else 4], sib).start()

    def qstep(r, half, way=None):
        org, at, ways, k = steps(r, way)
        if r == 4:
            at = at + c
        slot = ob.at[
            pl.ds(OZ // 2 * half, OZ // 2), pl.ds(pl.multiple_of((org * 2 + c) * GD, GD), GD)
        ]
        if at is not None:
            remote(slot, slot, zqsend.at[0], zqrecv.at[at * 2 + half], sib).wait_recv()

        def start(w):
            i = (r * 2 + w) * 2 + half
            remote(slot, slot, zqsend.at[0], zqrecv.at[i], toz[w]).start()

        onward(r, ways, start, alternate)
        remote(slot, slot, bsend.at[2], brecv.at[2], sib).start()

    def pslot(group, chip):
        rows = pl.ds(pl.multiple_of(OZ + OQ * group, 16), OQ)
        return ob.at[rows, pl.ds(pl.multiple_of((chip * 2 + c) * GD, GD), GD)]

    def pstep(r, way=None):
        org, at, ways, k = steps(r, way)
        if r == 4:
            at = at + c
        slot = pslot(y, org)
        if at is not None:
            remote(slot, slot, zpsend.at[0], zprecv.at[at], sib).wait_recv()

        def start(w):
            i = r * 2 + w
            remote(slot, slot, zpsend.at[0], zprecv.at[i], toz[w]).start()

        onward(r, ways, start, alternate)
        for w in range(2):
            remote(slot, slot, oysend.at[0], oyrecv.at[w * 8 + k], toy[w]).start()
        remote(slot, slot, bsend.at[3], brecv.at[3], sib).start()

    def pystep(a, k):
        slot = pslot(ygroup(a), kchip(k))
        remote(slot, slot, oysend.at[0], oyrecv.at[a * 8 + k], sib).wait_recv()
        if a < 2:
            @pl.when(c == a)
            def _():
                remote(slot, slot, oysend.at[0], oyrecv.at[16 + k], toy[a]).start()
        remote(slot, slot, bsend.at[3], brecv.at[3], sib).start()

    def yrun(fn, ks, ways):
        for k in ks:
            for a in ways:
                fn(a, k)

    def mpair(r):
        mstep(r, 0)
        mstep(r, 1)

    def wpair(r):
        for half in range(2):
            wstep(r, half, 0)
            wstep(r, half, 1)

    def qpair(r):
        for half in range(2):
            qstep(r, half, 0)
            qstep(r, half, 1)

    def ppair(r):
        pstep(r, 0)
        pstep(r, 1)

    def spread_bias(j, _):
        bt[j] = jnp.transpose(jnp.broadcast_to(sb[j], (GD, SPAN)))
        return 0

    def activate(up, gate, jj, start, n):
        for i in range(2):
            j = 2 * jj + i
            u = up[:, i * GD:(i + 1) * GD].astype(bf16).astype(f32)
            op[j, pl.ds(start, n), :] = gelu(u)
            a = gelu(gate[:, i * GD:(i + 1) * GD].astype(bf16).astype(f32))
            a = a - jnp.mean(a, axis=-1, keepdims=True)
            spread = jnp.mean(a * a, axis=-1, keepdims=True)
            v[j, pl.ds(start, n), :] = (a * lax.rsqrt(spread + norm_eps) * sg[j]).astype(bf16)

    def wcols(half, jj):
        return pl.ds(pl.multiple_of(512 * half + jj * 256, 256), 256)

    def project(xs, row=0, n=ROWS, pairs=(0, 2)):
        start = pl.multiple_of(xs * ROWS + row, 16)

        def pair(jj, _):
            t = tok[xs, row:row + n, :]
            up = jnp.dot(t, wb[:, wcols(0, jj)], preferred_element_type=f32)
            gate = jnp.dot(t, wb[:, wcols(1, jj)], preferred_element_type=f32)
            activate(up, gate, jj, start, n)
            return 0

        lax.fori_loop(*pairs, pair, 0)

    def over_chips(xs, chips, half, jj):
        total = None
        for chip in chips:
            rows = pl.ds(pl.multiple_of(chip * 256, 256), 256)
            p = jnp.dot(tok[xs, :, rows], wb[rows, wcols(half, jj)], preferred_element_type=f32)
            total = p if total is None else total + p
        return total

    near = [z] + [zorg(r, w) for r in (1, 2) for w in range(2)]
    far = [zorg(3, 0), zorg(3, 1), mod(z + 4, NZ)]

    def project_near(xs, i):
        def tile(k, _):
            half, jj = lax.div(k, 2), lax.rem(k, 2)
            pa[i, :, wcols(half, jj)] = over_chips(xs, near, half, jj)
            return 0

        lax.fori_loop(0, 4, tile, 0)

    def project_far(xs, i):
        start = pl.multiple_of(xs * ROWS, 16)

        def pair(jj, _):
            up = pa[i, :, wcols(0, jj)] + over_chips(xs, far, 0, jj)
            gate = pa[i, :, wcols(1, jj)] + over_chips(xs, far, 1, jj)
            activate(up, gate, jj, start, ROWS)
            return 0

        lax.fori_loop(0, 2, pair, 0)

    def wait_all(ref, i):
        remote(ref, ref, bsend.at[i], brecv.at[i], sib).wait_recv()

    mstep(0)
    for k in range(XN):
        for w in range(2):
            remote(xslot(x, k), xslot(x, k), xsend.at[0], xrecv.at[w * XN + k], tox[w]).start()
    wstep(0, 0)
    wstep(0, 1)
    for k in (1, 2, 3):
        peer = dev(x, mod(y + k, NY), z, c)
        remote(sb.at[y], sb.at[y], ssend.at[0], srecv.at[0], peer).start()
        remote(sg.at[y], sg.at[y], ssend.at[1], srecv.at[1], peer).start()

    mpair(1)
    yrun(ystep, (0,), (0, 1))
    wpair(1)
    mpair(2)
    yrun(ystep, (1, 2), (0, 1))
    xforward(0)
    remote(sb.at[0:3], sb.at[0:3], ssend.at[0], srecv.at[0], sib).wait_recv()
    remote(sg.at[0:3], sg.at[0:3], ssend.at[1], srecv.at[1], sib).wait_recv()
    lax.fori_loop(0, 4, spread_bias, 0)
    wpair(2)
    yrun(ystep, (0,), (2,))
    mpair(3)
    xforward(1)
    yrun(ystep, (3, 4), (0, 1))
    wait_all(wb.at[0:640, :], 1)
    project_near(x, 0)
    wpair(3)
    pstep(0)
    qstep(0, 0)
    qstep(0, 1)
    mstep(4)
    xforward(2)
    yrun(ystep, (5, 6), (0, 1))
    yrun(ystep, (1, 2), (2,))
    xforward(3)
    project_near(xfrom1, 1)
    wstep(4, 0)
    wstep(4, 1)


    xother = mod(x + 1 + 2 * c, NX)
    for k in range(XN):
        slot = xslot(xother, k)
        remote(slot, slot, xsend.at[0], xrecv.at[(1 - c) * XN + k], sib).wait_recv()
    project_near(xother, 2)
    wait_all(wb.at[0:384, :], 4)
    project_far(x, 0)
    yrun(ystep, (7,), (0, 1))
    ppair(1)
    yrun(pystep, (0,), (0, 1))
    yrun(ystep, (3, 4), (2,))
    project_far(xfrom1, 1)
    qpair(1)
    yrun(ystep, (5, 6), (2,))
    project_far(xother, 2)

    def xlast(k):
        slot = xslot(xfrom2, k)
        remote(slot, slot, xsend.at[0], xrecv.at[2 * XN + k], sib).wait_recv()

    for k in range(XN - 1):
        xlast(k)
    project(xfrom2, 0, ROWS - XR)
    ppair(2)
    yrun(ystep, (7,), (2,))

    for cc in range(2):
        @pl.when(c != cc)
        def _():
            wait_all(mb.at[:, 0:MSUM[cc], :], 0)

    xlast(XN - 1)
    project(xfrom2, ROWS - XR, XR, (0, 1))

    kmax = (384, 640, 1024, 1280)
    kfree = (0, 256, 640, 896)

    def lanes(j, xx):
        return pl.ds(pl.multiple_of((4 * j + xx) * GD, GD), GD)

    def acopy(j, r):
        src = g.at[j, pl.ds(ROWS * r, ROWS), :]
        return remote(src, ab.at[:, lanes(j, x)], asend.at[0], arecv.at[j], dev(r, y, z, c))

    def alocal(j, r):
        src = g.at[j, pl.ds(ROWS * r, ROWS), :]
        return pltpu.make_async_copy(src, ab.at[:, lanes(j, x)], asem.at[0])

    def mix(j, _):
        for r in range(4):
            rows = pl.ds(ROWS * r, ROWS)
            k0, k1 = kfree[r], kmax[r]
            at_row = lax.broadcasted_iota(jnp.int32, (ROWS, k1 - k0), 0) + ROWS * r
            at_col = lax.broadcasted_iota(jnp.int32, (ROWS, k1 - k0), 1) + k0
            edge = mb[j, rows, k0:k1].astype(f32)
            edge = jnp.where(at_col <= at_row, edge, 0.0).astype(bf16)
            total = jnp.dot(edge, v[j, k0:k1, :], preferred_element_type=f32)
            if k0:
                total += jnp.dot(
                    mb[j, rows, 0:k0], v[j, 0:k0, :], preferred_element_type=f32
                )
            g[j, rows, :] = (op[j, rows, :] * (total + bt[j, rows, :])).astype(bf16)

        for r in range(4):
            @pl.when(x != r)
            def _():
                acopy(j, r).start()

            @pl.when(x == r)
            def _():
                alocal(j, r).start()
        return 0

    lax.fori_loop(0, 1, mix, 0)
    yrun(pystep, (1, 2), (0, 1))
    lax.fori_loop(1, 2, mix, 0)
    ppair(3)
    qpair(2)
    project(xfrom2, ROWS - XR, XR, (1, 2))
    lax.fori_loop(2, 3, mix, 0)
    yrun(pystep, (3, 4), (0, 1))
    lax.fori_loop(3, 4, mix, 0)
    pstep(4)
    qstep(3, 0, 0)
    qstep(3, 0, 1)
    yrun(pystep, (5, 6), (0, 1))
    qstep(3, 1, 0)
    qstep(3, 1, 1)
    yrun(pystep, (0, 1, 2), (2,))
    yrun(pystep, (7,), (0, 1))
    yrun(pystep, (3, 4), (2,))
    qstep(4, 0)
    qstep(4, 1)
    yrun(pystep, (5, 6), (2,))

    pltpu.make_async_copy(ab.at[:, 0:4 * GD], ab.at[:, 0:4 * GD], asem.at[0]).wait()

    def partial_out(j):
        slot = ab.at[:, 0:3 * GD]
        remote(slot, slot, asend.at[0], arecv.at[j], sib).wait_recv()
        k0 = 512 * j

        def prepare(i, _):
            rows = pl.ds(pl.multiple_of(i * 64, 16), 64)
            squares = jnp.zeros((64, GD), f32)
            for k in range(k0, k0 + 512, GD):
                a = ab[rows, k:k + GD].astype(f32)
                squares += a * a
                nb[rows, k:k + GD] = (a * og[:, k:k + GD]).astype(bf16)
            if j:
                squares += ss[rows, :]
            ss[rows, :] = squares
            return 0

        lax.fori_loop(0, ROWS // 64, prepare, 0)
        if j == 3:
            mean = jnp.sum(ss[...], axis=-1, keepdims=True) * (1.0 / WIDTH)
            scale = lax.rsqrt(mean + norm_eps)

        def product(i, _):
            cols = pl.ds(pl.multiple_of(i * 1024, 1024), 1024)
            p = jnp.dot(nb[:, k0:k0 + 512], ob[k0:k0 + 512, cols], preferred_element_type=f32)
            if j:
                p += acc[:, cols]
            if j < 3:
                acc[:, cols] = p
            else:
                ov[:, cols] = (p * scale).astype(bf16)
                pltpu.make_async_copy(ov.at[:, cols], out_ref.at[0, :, cols], osem.at[0]).start()
            return 0

        lax.fori_loop(0, 2, product, 0)

    wait_all(ob.at[0:OZ, 0:1024], 2)
    partial_out(0)
    yrun(pystep, (7,), (2,))
    wait_all(ob.at[0:WIDTH - OZ, 0:1024], 3)
    partial_out(1)
    partial_out(2)
    partial_out(3)

    def sent(ref, sem):
        remote(ref, ref, sem, brecv.at[0], sib).wait_send()

    sent(sb.at[0:3], ssend.at[0])
    sent(sg.at[0:3], ssend.at[1])
    sent(tok.at[0:3], xsend.at[0])
    sent(wb.at[0:768, :], zwsend.at[0])
    for w in range(2):
        @pl.when(light[w])
        def _():
            sent(wb.at[0:GD, :], zwsend.at[1 + w])
    sent(ob.at[0:OZ, 0:896], zqsend.at[0])
    sent(ob.at[0:OQ, 0:896], zpsend.at[0])
    sent(ob.at[0:OQ * 2, 0:1536], oysend.at[0])
    sent(wb.at[0:1024, :], bsend.at[1])
    sent(ob.at[0:OZ, 0:1024], bsend.at[2])
    sent(ob.at[0:WIDTH - OZ, 0:1024], bsend.at[3])
    sent(ab.at[:, 0:12 * GD], asend.at[0])
    for cc in range(2):
        @pl.when(c == cc)
        def _():
            sent(mb.at[:, 0:MSUM[cc], :], bsend.at[0])
            sent(mb.at[0:3, 0:MSUM[cc], :], ysend.at[0])

    def msent(i, _):
        r, w = lax.div(i, 2), lax.rem(i, 2)
        org = mod(z + lax.select(w == 0, NZ - r, r), NZ)

        def go(width):
            slot = mslot(y, org * 2 + c, width)
            remote(slot, slot, zmsend.at[i], zmrecv.at[0], sib).wait_send()

        @pl.when((i < 6) | ((i == 6) & light[0]) | ((i == 7) & light[1]))
        def _():
            by_width(org * 2 + c, go)
        return 0

    lax.fori_loop(0, 8, msent, 0)
    pltpu.make_async_copy(ov, out_ref.at[0], osem.at[0]).wait()


def body(tokens, up_weight, gate_weight, group_gain, mix_weight, mix_bias, out_gain, out_weight):
    hbm = pl.BlockSpec(memory_space=pltpu.HBM)
    dma = pltpu.SemaphoreType.DMA
    return pl.pallas_call(
        kernel,
        out_shape=jax.ShapeDtypeStruct((1, ROWS, WIDTH), bf16),
        in_specs=[hbm] * 8,
        out_specs=pl.BlockSpec(memory_space=pl.ANY),
        scratch_shapes=[
            pltpu.VMEM((NX, ROWS, WIDTH), bf16),
            pltpu.VMEM((WIDTH, 1024), bf16),
            pltpu.VMEM((4, SPAN, SPAN), bf16),
            pltpu.VMEM((WIDTH, WIDTH), bf16),
            pltpu.VMEM((4, SPAN, GD), bf16),
            pltpu.VMEM((4, SPAN, GD), f32),
            pltpu.VMEM((4, SPAN, GD), f32),
            pltpu.VMEM((4, SPAN, GD), bf16),
            pltpu.VMEM((ROWS, WIDTH), bf16),
            pltpu.VMEM((ROWS, WIDTH), bf16),
            pltpu.VMEM((4, 1, SPAN), f32),
            pltpu.VMEM((4, 1, GD), f32),
            dma((7,)),
            dma((1,)),
            dma((12,)),
            dma((8,)),
            dma((8,)),
            dma((3,)),
            dma((16,)),
            dma((1,)),
            dma((16,)),
            dma((1,)),
            dma((8,)),
            dma((1,)),
            dma((24,)),
            dma((1,)),
            dma((24,)),
            dma((4,)),
            dma((5,)),
            dma((1,)),
            dma((4,)),
            dma((2,)),
            dma((2,)),
            dma((1,)),
            dma((1,)),
            pltpu.VMEM((ROWS, WIDTH), bf16),
            pltpu.VMEM((1, WIDTH), f32),
            pltpu.VMEM((ROWS, WIDTH), f32),
            pltpu.VMEM((ROWS, GD), f32),
            pltpu.VMEM((3, ROWS, 1024), f32),
        ],
        compiler_params=pltpu.CompilerParams(
            collective_id=0, has_side_effects=True, vmem_limit_bytes=54_000_000
        ),
        name="gating",
    )(
        *(
            pltpu.with_memory_space_constraint(a, pltpu.HBM)
            for a in (
                tokens, up_weight, gate_weight, group_gain, mix_weight, mix_bias,
                out_gain.reshape(1, WIDTH), out_weight,
            )
        )
    )


def solution(mesh):
    return jax.shard_map(
        body,
        mesh=mesh,
        in_specs=(
            P("dp", "sp", None),
            P("dp", None),
            P("dp", None),
            P("sp", None),
            P("sp", "dp", None),
            P("sp", None),
            P(),
            P(None, "dp"),
        ),
        out_specs=P("dp", "sp", None),
        check_vma=False,
    )
```

```python
import functools

import jax
import jax.numpy as jnp
from jax import lax
from jax.experimental import pallas as pl
from jax.experimental.pallas import tpu as pltpu
from jax.sharding import PartitionSpec as P

norm_eps = 1e-06
NX, NY, NZ = 4, 4, 8
ROWS = 320
SPAN = 1280
WIDTH = 2048
GD = 128
MROWS = 80
OZ = 896
KA = min(OZ, 1024) // 256 * 256
OQ = (WIDTH - OZ) // 4
XN = 4
XR = ROWS // XN
MSUM = (352, 384)
f32 = jnp.float32
bf16 = jnp.bfloat16


def remote(src, dst, send, recv, dev):
    return pltpu.make_async_remote_copy(
        src_ref=src,
        dst_ref=dst,
        send_sem=send,
        recv_sem=recv,
        device_id=dev,
        device_id_type=pl.DeviceIdType.MESH,
    )


def gelu(a):
    return 0.5 * a * (1.0 + jnp.tanh(0.7978845608028654 * (a + 0.044715 * (a * a * a))))


def kernel(
    tokens, upw, gatew, gain, mixw, bias, ogain, outw, out_ref,
    tok, wb, mb, ob, v, op, bt, g, ab, nb, sb, sg,
    lsem, xsend, xrecv, zmsend, zmrecv, zwsend, zwrecv, zqsend, zqrecv,
    zpsend, zprecv, ysend, yrecv, oysend, oyrecv, bsend, brecv,
    asend, arecv, ssend, srecv, asem, osem, ov, og, acc, ss, pa,
):
    sp = lax.axis_index("sp")
    dp = lax.axis_index("dp")
    y, x = lax.div(sp, NX), lax.rem(sp, NX)
    z, c = lax.div(dp, 2), lax.rem(dp, 2)

    def dev(xx, yy, zz, cc):
        return {"sp": yy * NX + xx, "dp": zz * 2 + cc}

    def mod(a, n):
        return lax.rem(a, n)

    tox = [dev(mod(x + 1, NX), y, z, c), dev(mod(x + NX - 1, NX), y, z, c)]
    toy = [dev(x, mod(y + 1, NY), z, c), dev(x, mod(y + NY - 1, NY), z, c)]
    toz = [dev(x, y, mod(z + 1, NZ), c), dev(x, y, mod(z + NZ - 1, NZ), c)]
    sib = dev(x, y, z, 1 - c)

    def xorg(r, way):
        return mod(x + (NX - r if way == 0 else r), NX)

    def yorg(r, way):
        return mod(y + (NY - r if way == 0 else r), NY)

    def zorg(r, way):
        return mod(z + (NZ - r if way == 0 else r), NZ)

    d = z * 2 + c
    wrow = pl.ds(pl.multiple_of(d * GD, GD), GD)
    loads = [
        pltpu.make_async_copy(
            mixw.at[0], mb.at[y, pl.ds(pl.multiple_of(d * MROWS, 16), MROWS), :], lsem.at[1]
        ),
        pltpu.make_async_copy(tokens.at[0], tok.at[x], lsem.at[0]),
        pltpu.make_async_copy(outw, ob.at[:, wrow], lsem.at[2]),
        pltpu.make_async_copy(bias, sb.at[y], lsem.at[3]),
        pltpu.make_async_copy(gain, sg.at[y], lsem.at[4]),
        pltpu.make_async_copy(ogain, og, lsem.at[6]),
    ]
    for load in loads:
        load.start()
    for j in range(4):
        cols = pl.ds(pl.multiple_of((x + 4 * j) * GD, GD), GD)
        for half, w in enumerate((upw, gatew)):
            pltpu.make_async_copy(
                w.at[:, cols], wb.at[wrow, pl.ds(512 * half + j * GD, GD)], lsem.at[5]
            ).start()
    loads.append(pltpu.make_async_copy(wb.at[wrow, :], wb.at[wrow, :], lsem.at[5]))

    barrier = pltpu.get_barrier_semaphore()
    peers = [dev(mod(x + k, NX), y, z, c) for k in (1, 2, 3)]
    peers += [dev(x, mod(y + k, NY), z, c) for k in (1, 2, 3)]
    peers += toz + [sib]
    for peer in peers:
        pl.semaphore_signal(barrier, inc=1, device_id=peer, device_id_type=pl.DeviceIdType.MESH)
    pl.semaphore_wait(barrier, len(peers))
    for load in loads:
        load.wait()

    def xslot(shard, k):
        return tok.at[shard, pl.ds(k * XR, XR), :]

    xfrom1 = mod(x + NX - 1 + 2 * c, NX)
    xfrom2 = mod(x + 2, NX)
    xto = dev(mod(x + 1 + 2 * c, NX), y, z, c)

    def xforward(k):
        slot = xslot(xfrom1, k)
        remote(slot, slot, xsend.at[0], xrecv.at[c * XN + k], xto).wait_recv()
        remote(slot, slot, xsend.at[0], xrecv.at[2 * XN + k], xto).start()

    def by_width(dd, fn):
        n = lax.div(MROWS * (dd + 1) + GD - 1, GD)
        for k in range(1, 11):
            @pl.when(n == k)
            def _():
                fn(GD * k)

    def mslot(group, dd, width):
        return mb.at[group, pl.ds(pl.multiple_of(dd * MROWS, 16), MROWS), pl.ds(0, width)]

    def last_way(chip):
        return lax.div(mod(chip + 6, NZ), 4)

    light = [last_way(mod(z + 1, NZ)) == 0, last_way(mod(z + NZ - 1, NZ)) == 1]
    alternate = [c == 0, c == 1]

    def steps(r, way):
        if r == 0:
            return z, None, [0, 1], 0
        if r == 4:
            return mod(z + 4, NZ), 6, [], 7
        return zorg(r, way), (r - 1) * 2 + way, [way], 2 * r - 1 + way

    def onward(r, way, start, last):
        for w in way:
            if r < 3:
                start(w)
            else:
                @pl.when(last[w])
                def _():
                    start(w)

    def mstep(r, way=None):
        org, at, ways, k = steps(r, way)
        if r == 4:
            at = at + last_way(z)
        dd = org * 2 + c

        def go(width):
            slot = mslot(y, dd, width)
            if at is not None:
                remote(slot, slot, zmsend.at[0], zmrecv.at[at], sib).wait_recv()

            def start(w):
                i = r * 2 + w
                remote(slot, slot, zmsend.at[i], zmrecv.at[i], toz[w]).start()

            onward(r, ways, start, light)
            for w in range(2):
                remote(slot, slot, ysend.at[0], yrecv.at[w * 8 + k], toy[w]).start()
            remote(slot, slot, bsend.at[0], brecv.at[0], sib).start()

        by_width(dd, go)

    def ygroup(a):
        return mod(y + 2, NY) if a == 2 else yorg(1, a)

    def kchip(k):
        if k == 0:
            return z
        if k == 7:
            return mod(z + 4, NZ)
        return zorg((k + 1) // 2, (k + 1) % 2)

    def ystep(a, k):
        dd = kchip(k) * 2 + c

        def go(width):
            slot = mslot(ygroup(a), dd, width)
            remote(slot, slot, ysend.at[0], yrecv.at[a * 8 + k], sib).wait_recv()
            if a < 2:
                @pl.when(c == a)
                def _():
                    remote(slot, slot, ysend.at[0], yrecv.at[16 + k], toy[a]).start()
            remote(slot, slot, bsend.at[0], brecv.at[0], sib).start()

        by_width(dd, go)

    def wstep(r, half, way=None):
        org, at, ways, k = steps(r, way)
        if r == 4:
            at = at + last_way(z)
        slot = wb.at[
            pl.ds(pl.multiple_of((org * 2 + c) * GD, GD), GD), pl.ds(512 * half, 512)
        ]
        if at is not None:
            remote(slot, slot, zwsend.at[0], zwrecv.at[at * 2 + half], sib).wait_recv()

        def start(w):
            i = (r * 2 + w) * 2 + half
            remote(slot, slot, zwsend.at[0 if r < 3 else 1 + w], zwrecv.at[i], toz[w]).start()

        onward(r, ways, start, light)
        remote(slot, slot, bsend.at[1], brecv.at[1 if r < 3 else 4], sib).start()

    def qstep(r, half, way=None):
        org, at, ways, k = steps(r, way)
        if r == 4:
            at = at + c
        slot = ob.at[
            pl.ds(OZ // 2 * half, OZ // 2), pl.ds(pl.multiple_of((org * 2 + c) * GD, GD), GD)
        ]
        if at is not None:
            remote(slot, slot, zqsend.at[0], zqrecv.at[at * 2 + half], sib).wait_recv()

        def start(w):
            i = (r * 2 + w) * 2 + half
            remote(slot, slot, zqsend.at[0], zqrecv.at[i], toz[w]).start()

        onward(r, ways, start, alternate)
        remote(slot, slot, bsend.at[2], brecv.at[2], sib).start()

    def pslot(group, chip):
        rows = pl.ds(pl.multiple_of(OZ + OQ * group, 16), OQ)
        return ob.at[rows, pl.ds(pl.multiple_of((chip * 2 + c) * GD, GD), GD)]

    def pstep(r, way=None):
        org, at, ways, k = steps(r, way)
        if r == 4:
            at = at + c
        slot = pslot(y, org)
        if at is not None:
            remote(slot, slot, zpsend.at[0], zprecv.at[at], sib).wait_recv()

        def start(w):
            i = r * 2 + w
            remote(slot, slot, zpsend.at[0], zprecv.at[i], toz[w]).start()

        onward(r, ways, start, alternate)
        for w in range(2):
            remote(slot, slot, oysend.at[0], oyrecv.at[w * 8 + k], toy[w]).start()
        remote(slot, slot, bsend.at[3], brecv.at[3], sib).start()

    def pystep(a, k):
        slot = pslot(ygroup(a), kchip(k))
        remote(slot, slot, oysend.at[0], oyrecv.at[a * 8 + k], sib).wait_recv()
        if a < 2:
            @pl.when(c == a)
            def _():
                remote(slot, slot, oysend.at[0], oyrecv.at[16 + k], toy[a]).start()
        remote(slot, slot, bsend.at[3], brecv.at[3], sib).start()

    def yrun(fn, ks, ways):
        for k in ks:
            for a in ways:
                fn(a, k)

    def mpair(r):
        mstep(r, 0)
        mstep(r, 1)

    def wpair(r):
        for half in range(2):
            wstep(r, half, 0)
            wstep(r, half, 1)

    def qpair(r):
        for half in range(2):
            qstep(r, half, 0)
            qstep(r, half, 1)

    def ppair(r):
        pstep(r, 0)
        pstep(r, 1)

    def spread_bias(j, _):
        bt[j] = jnp.transpose(jnp.broadcast_to(sb[j], (GD, SPAN)))
        return 0

    def activate(up, gate, jj, start, n):
        for i in range(2):
            j = 2 * jj + i
            u = up[:, i * GD:(i + 1) * GD].astype(bf16).astype(f32)
            op[j, pl.ds(start, n), :] = gelu(u)
            a = gelu(gate[:, i * GD:(i + 1) * GD].astype(bf16).astype(f32))
            a = a - jnp.mean(a, axis=-1, keepdims=True)
            spread = jnp.mean(a * a, axis=-1, keepdims=True)
            v[j, pl.ds(start, n), :] = (a * lax.rsqrt(spread + norm_eps) * sg[j]).astype(bf16)

    def wcols(half, jj):
        return pl.ds(pl.multiple_of(512 * half + jj * 256, 256), 256)

    def project(xs, row=0, n=ROWS, pairs=(0, 2)):
        start = pl.multiple_of(xs * ROWS + row, 16)

        def pair(jj, _):
            t = tok[xs, row:row + n, :]
            up = jnp.dot(t, wb[:, wcols(0, jj)], preferred_element_type=f32)
            gate = jnp.dot(t, wb[:, wcols(1, jj)], preferred_element_type=f32)
            activate(up, gate, jj, start, n)
            return 0

        lax.fori_loop(*pairs, pair, 0)

    def over_chips(xs, chips, half, jj):
        total = None
        for chip in chips:
            rows = pl.ds(pl.multiple_of(chip * 256, 256), 256)
            p = jnp.dot(tok[xs, :, rows], wb[rows, wcols(half, jj)], preferred_element_type=f32)
            total = p if total is None else total + p
        return total

    near = [z] + [zorg(r, w) for r in (1, 2) for w in range(2)]
    far = [zorg(3, 0), zorg(3, 1), mod(z + 4, NZ)]

    def project_near(xs, i):
        def tile(k, _):
            half, jj = lax.div(k, 2), lax.rem(k, 2)
            pa[i, :, wcols(half, jj)] = over_chips(xs, near, half, jj)
            return 0

        lax.fori_loop(0, 4, tile, 0)

    def project_far(xs, i):
        start = pl.multiple_of(xs * ROWS, 16)

        def pair(jj, _):
            up = pa[i, :, wcols(0, jj)] + over_chips(xs, far, 0, jj)
            gate = pa[i, :, wcols(1, jj)] + over_chips(xs, far, 1, jj)
            activate(up, gate, jj, start, ROWS)
            return 0

        lax.fori_loop(0, 2, pair, 0)

    def wait_all(ref, i):
        remote(ref, ref, bsend.at[i], brecv.at[i], sib).wait_recv()

    mstep(0)
    for k in range(XN):
        for w in range(2):
            remote(xslot(x, k), xslot(x, k), xsend.at[0], xrecv.at[w * XN + k], tox[w]).start()
    wstep(0, 0)
    wstep(0, 1)
    for k in (1, 2, 3):
        peer = dev(x, mod(y + k, NY), z, c)
        remote(sb.at[y], sb.at[y], ssend.at[0], srecv.at[0], peer).start()
        remote(sg.at[y], sg.at[y], ssend.at[1], srecv.at[1], peer).start()

    mpair(1)
    yrun(ystep, (0,), (0, 1))
    wpair(1)
    mpair(2)
    yrun(ystep, (1, 2), (0, 1))
    xforward(0)
    remote(sb.at[0:3], sb.at[0:3], ssend.at[0], srecv.at[0], sib).wait_recv()
    remote(sg.at[0:3], sg.at[0:3], ssend.at[1], srecv.at[1], sib).wait_recv()
    lax.fori_loop(0, 4, spread_bias, 0)
    wpair(2)
    yrun(ystep, (0,), (2,))
    mpair(3)
    xforward(1)
    yrun(ystep, (3, 4), (0, 1))
    wait_all(wb.at[0:640, :], 1)
    project_near(x, 0)
    wpair(3)
    pstep(0)
    qstep(0, 0)
    qstep(0, 1)
    mstep(4)
    xforward(2)
    yrun(ystep, (5, 6), (0, 1))
    yrun(ystep, (1, 2), (2,))
    xforward(3)
    project_near(xfrom1, 1)
    wstep(4, 0)
    wstep(4, 1)


    xother = mod(x + 1 + 2 * c, NX)
    for k in range(XN):
        slot = xslot(xother, k)
        remote(slot, slot, xsend.at[0], xrecv.at[(1 - c) * XN + k], sib).wait_recv()
    project_near(xother, 2)
    wait_all(wb.at[0:384, :], 4)
    project_far(x, 0)
    yrun(ystep, (7,), (0, 1))
    ppair(1)
    yrun(pystep, (0,), (0, 1))
    yrun(ystep, (3, 4), (2,))
    project_far(xfrom1, 1)
    qpair(1)
    yrun(ystep, (5, 6), (2,))
    project_far(xother, 2)

    def xlast(k):
        slot = xslot(xfrom2, k)
        remote(slot, slot, xsend.at[0], xrecv.at[2 * XN + k], sib).wait_recv()

    for k in range(XN - 1):
        xlast(k)
    project(xfrom2, 0, ROWS - XR, (0, 1))
    ppair(2)
    yrun(ystep, (7,), (2,))
    project(xfrom2, 0, ROWS - XR, (1, 2))

    xlast(XN - 1)
    project(xfrom2, ROWS - XR, XR, (0, 1))

    for cc in range(2):
        @pl.when(c != cc)
        def _():
            wait_all(mb.at[:, 0:MSUM[cc], :], 0)

    kmax = (384, 640, 1024, 1280)
    kfree = (0, 256, 640, 896)

    def lanes(j, xx):
        return pl.ds(pl.multiple_of((4 * j + xx) * GD, GD), GD)

    def acopy(j, r):
        src = g.at[j, pl.ds(ROWS * r, ROWS), :]
        return remote(src, ab.at[:, lanes(j, x)], asend.at[0], arecv.at[j], dev(r, y, z, c))

    def alocal(j, r):
        src = g.at[j, pl.ds(ROWS * r, ROWS), :]
        return pltpu.make_async_copy(src, ab.at[:, lanes(j, x)], asem.at[0])

    def mix(j, _):
        for r in range(4):
            rows = pl.ds(ROWS * r, ROWS)
            k0, k1 = kfree[r], kmax[r]
            at_row = lax.broadcasted_iota(jnp.int32, (ROWS, k1 - k0), 0) + ROWS * r
            at_col = lax.broadcasted_iota(jnp.int32, (ROWS, k1 - k0), 1) + k0
            edge = mb[j, rows, k0:k1].astype(f32)
            edge = jnp.where(at_col <= at_row, edge, 0.0).astype(bf16)
            total = jnp.dot(edge, v[j, k0:k1, :], preferred_element_type=f32)
            if k0:
                total += jnp.dot(
                    mb[j, rows, 0:k0], v[j, 0:k0, :], preferred_element_type=f32
                )
            g[j, rows, :] = (op[j, rows, :] * (total + bt[j, rows, :])).astype(bf16)

        for r in range(4):
            @pl.when(x != r)
            def _():
                acopy(j, r).start()

            @pl.when(x == r)
            def _():
                alocal(j, r).start()
        return 0

    lax.fori_loop(0, 1, mix, 0)
    yrun(pystep, (1, 2), (0, 1))
    lax.fori_loop(1, 2, mix, 0)
    qstep(2, 0, 0)
    qstep(2, 0, 1)
    project(xfrom2, ROWS - XR, XR, (1, 2))
    lax.fori_loop(2, 3, mix, 0)
    ppair(3)
    qstep(2, 1, 0)
    qstep(2, 1, 1)
    yrun(pystep, (3, 4), (0, 1))
    lax.fori_loop(3, 4, mix, 0)
    pstep(4)
    qstep(3, 0, 0)
    qstep(3, 0, 1)
    yrun(pystep, (5, 6), (0, 1))
    qstep(3, 1, 0)
    qstep(3, 1, 1)
    yrun(pystep, (0, 1, 2), (2,))
    yrun(pystep, (7,), (0, 1))
    yrun(pystep, (3, 4), (2,))
    qstep(4, 0)
    qstep(4, 1)
    yrun(pystep, (5, 6), (2,))

    pltpu.make_async_copy(ab.at[:, 0:4 * GD], ab.at[:, 0:4 * GD], asem.at[0]).wait()

    def prepare(j):
        slot = ab.at[:, 0:3 * GD]
        remote(slot, slot, asend.at[0], arecv.at[j], sib).wait_recv()

        def piece(i, _):
            rows = pl.ds(pl.multiple_of(i * 64, 16), 64)
            squares = jnp.zeros((64, GD), f32)
            for k in range(512 * j, 512 * j + 512, GD):
                a = ab[rows, k:k + GD].astype(f32)
                squares += a * a
                nb[rows, k:k + GD] = (a * og[:, k:k + GD]).astype(bf16)
            if j:
                squares += ss[rows, :]
            ss[rows, :] = squares
            return 0

        lax.fori_loop(0, ROWS // 64, piece, 0)

    def partial_out(k0, k1):
        if k1 == WIDTH:
            mean = jnp.sum(ss[...], axis=-1, keepdims=True) * (1.0 / WIDTH)
            scale = lax.rsqrt(mean + norm_eps)

        def product(i, _):
            cols = pl.ds(pl.multiple_of(i * 1024, 1024), 1024)
            p = jnp.dot(nb[:, k0:k1], ob[k0:k1, cols], preferred_element_type=f32)
            if k0:
                p += acc[:, cols]
            if k1 < WIDTH:
                acc[:, cols] = p
            else:
                ov[:, cols] = (p * scale).astype(bf16)
                pltpu.make_async_copy(ov.at[:, cols], out_ref.at[0, :, cols], osem.at[0]).start()
            return 0

        lax.fori_loop(0, 2, product, 0)

    def msent(i, _):
        r, w = lax.div(i, 2), lax.rem(i, 2)
        org = mod(z + lax.select(w == 0, NZ - r, r), NZ)

        def go(width):
            slot = mslot(y, org * 2 + c, width)
            remote(slot, slot, zmsend.at[i], zmrecv.at[0], sib).wait_send()

        @pl.when((i < 6) | ((i == 6) & light[0]) | ((i == 7) & light[1]))
        def _():
            by_width(org * 2 + c, go)
        return 0

    lax.fori_loop(0, 8, msent, 0)
    prepare(0)
    prepare(1)
    wait_all(ob.at[0:OZ, 0:1024], 2)
    yrun(pystep, (7,), (2,))
    partial_out(0, KA)
    prepare(2)
    wait_all(ob.at[0:WIDTH - OZ, 0:1024], 3)
    partial_out(KA, 1536)
    prepare(3)
    partial_out(1536, WIDTH)

    def sent(ref, sem):
        remote(ref, ref, sem, brecv.at[0], sib).wait_send()

    sent(sb.at[0:3], ssend.at[0])
    sent(sg.at[0:3], ssend.at[1])
    sent(tok.at[0:3], xsend.at[0])
    sent(wb.at[0:768, :], zwsend.at[0])
    for w in range(2):
        @pl.when(light[w])
        def _():
            sent(wb.at[0:GD, :], zwsend.at[1 + w])
    sent(ob.at[0:OZ, 0:896], zqsend.at[0])
    sent(ob.at[0:OQ, 0:896], zpsend.at[0])
    sent(ob.at[0:OQ * 2, 0:1536], oysend.at[0])
    sent(wb.at[0:1024, :], bsend.at[1])
    sent(ob.at[0:OZ, 0:1024], bsend.at[2])
    sent(ob.at[0:WIDTH - OZ, 0:1024], bsend.at[3])
    sent(ab.at[:, 0:12 * GD], asend.at[0])
    for cc in range(2):
        @pl.when(c == cc)
        def _():
            sent(mb.at[:, 0:MSUM[cc], :], bsend.at[0])
            sent(mb.at[0:3, 0:MSUM[cc], :], ysend.at[0])

    pltpu.make_async_copy(ov, out_ref.at[0], osem.at[0]).wait()


def body(tokens, up_weight, gate_weight, group_gain, mix_weight, mix_bias, out_gain, out_weight):
    hbm = pl.BlockSpec(memory_space=pltpu.HBM)
    dma = pltpu.SemaphoreType.DMA
    return pl.pallas_call(
        kernel,
        out_shape=jax.ShapeDtypeStruct((1, ROWS, WIDTH), bf16),
        in_specs=[hbm] * 8,
        out_specs=pl.BlockSpec(memory_space=pl.ANY),
        scratch_shapes=[
            pltpu.VMEM((NX, ROWS, WIDTH), bf16),
            pltpu.VMEM((WIDTH, 1024), bf16),
            pltpu.VMEM((4, SPAN, SPAN), bf16),
            pltpu.VMEM((WIDTH, WIDTH), bf16),
            pltpu.VMEM((4, SPAN, GD), bf16),
            pltpu.VMEM((4, SPAN, GD), f32),
            pltpu.VMEM((4, SPAN, GD), f32),
            pltpu.VMEM((4, SPAN, GD), bf16),
            pltpu.VMEM((ROWS, WIDTH), bf16),
            pltpu.VMEM((ROWS, WIDTH), bf16),
            pltpu.VMEM((4, 1, SPAN), f32),
            pltpu.VMEM((4, 1, GD), f32),
            dma((7,)),
            dma((1,)),
            dma((12,)),
            dma((8,)),
            dma((8,)),
            dma((3,)),
            dma((16,)),
            dma((1,)),
            dma((16,)),
            dma((1,)),
            dma((8,)),
            dma((1,)),
            dma((24,)),
            dma((1,)),
            dma((24,)),
            dma((4,)),
            dma((5,)),
            dma((1,)),
            dma((4,)),
            dma((2,)),
            dma((2,)),
            dma((1,)),
            dma((1,)),
            pltpu.VMEM((ROWS, WIDTH), bf16),
            pltpu.VMEM((1, WIDTH), f32),
            pltpu.VMEM((ROWS, WIDTH), f32),
            pltpu.VMEM((ROWS, GD), f32),
            pltpu.VMEM((3, ROWS, 1024), f32),
        ],
        compiler_params=pltpu.CompilerParams(
            collective_id=0, has_side_effects=True, vmem_limit_bytes=54_000_000
        ),
        name="gating",
    )(
        *(
            pltpu.with_memory_space_constraint(a, pltpu.HBM)
            for a in (
                tokens, up_weight, gate_weight, group_gain, mix_weight, mix_bias,
                out_gain.reshape(1, WIDTH), out_weight,
            )
        )
    )


def solution(mesh):
    return jax.shard_map(
        body,
        mesh=mesh,
        in_specs=(
            P("dp", "sp", None),
            P("dp", None),
            P("dp", None),
            P("sp", None),
            P("sp", "dp", None),
            P("sp", None),
            P(),
            P(None, "dp"),
        ),
        out_specs=P("dp", "sp", None),
        check_vma=False,
    )
```

```python
import functools

import jax
import jax.numpy as jnp
from jax import lax
from jax.experimental import pallas as pl
from jax.experimental.pallas import tpu as pltpu
from jax.sharding import PartitionSpec as P

norm_eps = 1e-06
NX, NY, NZ = 4, 4, 8
ROWS = 320
SPAN = 1280
WIDTH = 2048
GD = 128
MROWS = 80
OZ = 832
KA = min(OZ, 1024) // 256 * 256
OQ = (WIDTH - OZ) // 4
XN = 4
XR = ROWS // XN
MSUM = (352, 384)
f32 = jnp.float32
bf16 = jnp.bfloat16


def remote(src, dst, send, recv, dev):
    return pltpu.make_async_remote_copy(
        src_ref=src,
        dst_ref=dst,
        send_sem=send,
        recv_sem=recv,
        device_id=dev,
        device_id_type=pl.DeviceIdType.MESH,
    )


def gelu(a):
    return 0.5 * a * (1.0 + jnp.tanh(0.7978845608028654 * (a + 0.044715 * (a * a * a))))


def kernel(
    tokens, upw, gatew, gain, mixw, bias, ogain, outw, out_ref,
    tok, wb, mb, ob, v, op, bt, g, ab, nb, sb, sg,
    lsem, xsend, xrecv, zmsend, zmrecv, zwsend, zwrecv, zqsend, zqrecv,
    zpsend, zprecv, ysend, yrecv, oysend, oyrecv, bsend, brecv,
    asend, arecv, ssend, srecv, asem, osem, ov, og, acc, ss, pa,
):
    sp = lax.axis_index("sp")
    dp = lax.axis_index("dp")
    y, x = lax.div(sp, NX), lax.rem(sp, NX)
    z, c = lax.div(dp, 2), lax.rem(dp, 2)

    def dev(xx, yy, zz, cc):
        return {"sp": yy * NX + xx, "dp": zz * 2 + cc}

    def mod(a, n):
        return lax.rem(a, n)

    tox = [dev(mod(x + 1, NX), y, z, c), dev(mod(x + NX - 1, NX), y, z, c)]
    toy = [dev(x, mod(y + 1, NY), z, c), dev(x, mod(y + NY - 1, NY), z, c)]
    toz = [dev(x, y, mod(z + 1, NZ), c), dev(x, y, mod(z + NZ - 1, NZ), c)]
    sib = dev(x, y, z, 1 - c)

    def xorg(r, way):
        return mod(x + (NX - r if way == 0 else r), NX)

    def yorg(r, way):
        return mod(y + (NY - r if way == 0 else r), NY)

    def zorg(r, way):
        return mod(z + (NZ - r if way == 0 else r), NZ)

    d = z * 2 + c
    wrow = pl.ds(pl.multiple_of(d * GD, GD), GD)
    loads = [
        pltpu.make_async_copy(
            mixw.at[0], mb.at[y, pl.ds(pl.multiple_of(d * MROWS, 16), MROWS), :], lsem.at[1]
        ),
        pltpu.make_async_copy(tokens.at[0], tok.at[x], lsem.at[0]),
        pltpu.make_async_copy(outw, ob.at[:, wrow], lsem.at[2]),
        pltpu.make_async_copy(bias, sb.at[y], lsem.at[3]),
        pltpu.make_async_copy(gain, sg.at[y], lsem.at[4]),
        pltpu.make_async_copy(ogain, og, lsem.at[6]),
    ]
    for load in loads:
        load.start()
    for j in range(4):
        cols = pl.ds(pl.multiple_of((x + 4 * j) * GD, GD), GD)
        for half, w in enumerate((upw, gatew)):
            pltpu.make_async_copy(
                w.at[:, cols], wb.at[wrow, pl.ds(512 * half + j * GD, GD)], lsem.at[5]
            ).start()
    loads.append(pltpu.make_async_copy(wb.at[wrow, :], wb.at[wrow, :], lsem.at[5]))

    barrier = pltpu.get_barrier_semaphore()
    peers = [dev(mod(x + k, NX), y, z, c) for k in (1, 2, 3)]
    peers += [dev(x, mod(y + k, NY), z, c) for k in (1, 2, 3)]
    peers += toz + [sib]
    for peer in peers:
        pl.semaphore_signal(barrier, inc=1, device_id=peer, device_id_type=pl.DeviceIdType.MESH)
    pl.semaphore_wait(barrier, len(peers))
    for load in loads:
        load.wait()

    def xslot(shard, k):
        return tok.at[shard, pl.ds(k * XR, XR), :]

    xfrom1 = mod(x + NX - 1 + 2 * c, NX)
    xfrom2 = mod(x + 2, NX)
    xto = dev(mod(x + 1 + 2 * c, NX), y, z, c)

    def xforward(k):
        slot = xslot(xfrom1, k)
        remote(slot, slot, xsend.at[0], xrecv.at[c * XN + k], xto).wait_recv()
        remote(slot, slot, xsend.at[0], xrecv.at[2 * XN + k], xto).start()

    def by_width(dd, fn):
        n = lax.div(MROWS * (dd + 1) + GD - 1, GD)
        for k in range(1, 11):
            @pl.when(n == k)
            def _():
                fn(GD * k)

    def mslot(group, dd, width):
        return mb.at[group, pl.ds(pl.multiple_of(dd * MROWS, 16), MROWS), pl.ds(0, width)]

    def last_way(chip):
        return lax.div(mod(chip + 6, NZ), 4)

    light = [last_way(mod(z + 1, NZ)) == 0, last_way(mod(z + NZ - 1, NZ)) == 1]
    alternate = [c == 0, c == 1]

    def steps(r, way):
        if r == 0:
            return z, None, [0, 1], 0
        if r == 4:
            return mod(z + 4, NZ), 6, [], 7
        return zorg(r, way), (r - 1) * 2 + way, [way], 2 * r - 1 + way

    def onward(r, way, start, last):
        for w in way:
            if r < 3:
                start(w)
            else:
                @pl.when(last[w])
                def _():
                    start(w)

    def mstep(r, way=None):
        org, at, ways, k = steps(r, way)
        if r == 4:
            at = at + last_way(z)
        dd = org * 2 + c

        def go(width):
            slot = mslot(y, dd, width)
            if at is not None:
                remote(slot, slot, zmsend.at[0], zmrecv.at[at], sib).wait_recv()

            def start(w):
                i = r * 2 + w
                remote(slot, slot, zmsend.at[i], zmrecv.at[i], toz[w]).start()

            onward(r, ways, start, light)
            for w in range(2):
                remote(slot, slot, ysend.at[0], yrecv.at[w * 8 + k], toy[w]).start()
            remote(slot, slot, bsend.at[0], brecv.at[0], sib).start()

        by_width(dd, go)

    def ygroup(a):
        return mod(y + 2, NY) if a == 2 else yorg(1, a)

    def kchip(k):
        if k == 0:
            return z
        if k == 7:
            return mod(z + 4, NZ)
        return zorg((k + 1) // 2, (k + 1) % 2)

    def ystep(a, k):
        dd = kchip(k) * 2 + c

        def go(width):
            slot = mslot(ygroup(a), dd, width)
            remote(slot, slot, ysend.at[0], yrecv.at[a * 8 + k], sib).wait_recv()
            if a < 2:
                @pl.when(c == a)
                def _():
                    remote(slot, slot, ysend.at[0], yrecv.at[16 + k], toy[a]).start()
            remote(slot, slot, bsend.at[0], brecv.at[0], sib).start()

        by_width(dd, go)

    def wstep(r, half, way=None):
        org, at, ways, k = steps(r, way)
        if r == 4:
            at = at + last_way(z)
        slot = wb.at[
            pl.ds(pl.multiple_of((org * 2 + c) * GD, GD), GD), pl.ds(512 * half, 512)
        ]
        if at is not None:
            remote(slot, slot, zwsend.at[0], zwrecv.at[at * 2 + half], sib).wait_recv()

        def start(w):
            i = (r * 2 + w) * 2 + half
            remote(slot, slot, zwsend.at[0 if r < 3 else 1 + w], zwrecv.at[i], toz[w]).start()

        onward(r, ways, start, light)
        remote(slot, slot, bsend.at[1], brecv.at[1 if r < 3 else 4], sib).start()

    def qstep(r, half, way=None):
        org, at, ways, k = steps(r, way)
        if r == 4:
            at = at + c
        slot = ob.at[
            pl.ds(OZ // 2 * half, OZ // 2), pl.ds(pl.multiple_of((org * 2 + c) * GD, GD), GD)
        ]
        if at is not None:
            remote(slot, slot, zqsend.at[0], zqrecv.at[at * 2 + half], sib).wait_recv()

        def start(w):
            i = (r * 2 + w) * 2 + half
            remote(slot, slot, zqsend.at[0], zqrecv.at[i], toz[w]).start()

        onward(r, ways, start, alternate)
        remote(slot, slot, bsend.at[2], brecv.at[2], sib).start()

    def pslot(group, chip):
        rows = pl.ds(pl.multiple_of(OZ + OQ * group, 16), OQ)
        return ob.at[rows, pl.ds(pl.multiple_of((chip * 2 + c) * GD, GD), GD)]

    def pstep(r, way=None):
        org, at, ways, k = steps(r, way)
        if r == 4:
            at = at + c
        slot = pslot(y, org)
        if at is not None:
            remote(slot, slot, zpsend.at[0], zprecv.at[at], sib).wait_recv()

        def start(w):
            i = r * 2 + w
            remote(slot, slot, zpsend.at[0], zprecv.at[i], toz[w]).start()

        onward(r, ways, start, alternate)
        for w in range(2):
            remote(slot, slot, oysend.at[0], oyrecv.at[w * 8 + k], toy[w]).start()
        remote(slot, slot, bsend.at[3], brecv.at[3], sib).start()

    def pystep(a, k):
        slot = pslot(ygroup(a), kchip(k))
        remote(slot, slot, oysend.at[0], oyrecv.at[a * 8 + k], sib).wait_recv()
        if a < 2:
            @pl.when(c == a)
            def _():
                remote(slot, slot, oysend.at[0], oyrecv.at[16 + k], toy[a]).start()
        remote(slot, slot, bsend.at[3], brecv.at[3], sib).start()

    def yrun(fn, ks, ways):
        for k in ks:
            for a in ways:
                fn(a, k)

    def mpair(r):
        mstep(r, 0)
        mstep(r, 1)

    def wpair(r):
        for half in range(2):
            wstep(r, half, 0)
            wstep(r, half, 1)

    def qpair(r):
        for half in range(2):
            qstep(r, half, 0)
            qstep(r, half, 1)

    def ppair(r):
        pstep(r, 0)
        pstep(r, 1)

    def spread_bias(j, _):
        bt[j] = jnp.transpose(jnp.broadcast_to(sb[j], (GD, SPAN)))
        return 0

    def activate(up, gate, jj, start, n):
        for i in range(2):
            j = 2 * jj + i
            u = up[:, i * GD:(i + 1) * GD].astype(bf16).astype(f32)
            op[j, pl.ds(start, n), :] = gelu(u)
            a = gelu(gate[:, i * GD:(i + 1) * GD].astype(bf16).astype(f32))
            a = a - jnp.mean(a, axis=-1, keepdims=True)
            spread = jnp.mean(a * a, axis=-1, keepdims=True)
            v[j, pl.ds(start, n), :] = (a * lax.rsqrt(spread + norm_eps) * sg[j]).astype(bf16)

    def wcols(half, jj):
        return pl.ds(pl.multiple_of(512 * half + jj * 256, 256), 256)

    def project(xs, row=0, n=ROWS, pairs=(0, 2)):
        start = pl.multiple_of(xs * ROWS + row, 16)

        def pair(jj, _):
            t = tok[xs, row:row + n, :]
            up = jnp.dot(t, wb[:, wcols(0, jj)], preferred_element_type=f32)
            gate = jnp.dot(t, wb[:, wcols(1, jj)], preferred_element_type=f32)
            activate(up, gate, jj, start, n)
            return 0

        lax.fori_loop(*pairs, pair, 0)

    def over_chips(xs, chips, half, jj):
        total = None
        for chip in chips:
            rows = pl.ds(pl.multiple_of(chip * 256, 256), 256)
            p = jnp.dot(tok[xs, :, rows], wb[rows, wcols(half, jj)], preferred_element_type=f32)
            total = p if total is None else total + p
        return total

    near = [z] + [zorg(r, w) for r in (1, 2) for w in range(2)]
    far = [zorg(3, 0), zorg(3, 1), mod(z + 4, NZ)]

    def project_near(xs, i):
        def tile(k, _):
            half, jj = lax.div(k, 2), lax.rem(k, 2)
            pa[i, :, wcols(half, jj)] = over_chips(xs, near, half, jj)
            return 0

        lax.fori_loop(0, 4, tile, 0)

    def project_far(xs, i):
        start = pl.multiple_of(xs * ROWS, 16)

        def pair(jj, _):
            up = pa[i, :, wcols(0, jj)] + over_chips(xs, far, 0, jj)
            gate = pa[i, :, wcols(1, jj)] + over_chips(xs, far, 1, jj)
            activate(up, gate, jj, start, ROWS)
            return 0

        lax.fori_loop(0, 2, pair, 0)

    def wait_all(ref, i):
        remote(ref, ref, bsend.at[i], brecv.at[i], sib).wait_recv()

    mstep(0)
    for k in range(XN):
        for w in range(2):
            remote(xslot(x, k), xslot(x, k), xsend.at[0], xrecv.at[w * XN + k], tox[w]).start()
    wstep(0, 0)
    wstep(0, 1)
    for k in (1, 2, 3):
        peer = dev(x, mod(y + k, NY), z, c)
        remote(sb.at[y], sb.at[y], ssend.at[0], srecv.at[0], peer).start()
        remote(sg.at[y], sg.at[y], ssend.at[1], srecv.at[1], peer).start()

    mpair(1)
    yrun(ystep, (0,), (0, 1))
    wpair(1)
    mpair(2)
    yrun(ystep, (1, 2), (0, 1))
    xforward(0)
    remote(sb.at[0:3], sb.at[0:3], ssend.at[0], srecv.at[0], sib).wait_recv()
    remote(sg.at[0:3], sg.at[0:3], ssend.at[1], srecv.at[1], sib).wait_recv()
    lax.fori_loop(0, 4, spread_bias, 0)
    wpair(2)
    yrun(ystep, (0,), (2,))
    mpair(3)
    xforward(1)
    yrun(ystep, (3, 4), (0, 1))
    wait_all(wb.at[0:640, :], 1)
    project_near(x, 0)
    wpair(3)
    pstep(0)
    qstep(0, 0)
    qstep(0, 1)
    mstep(4)
    xforward(2)
    yrun(ystep, (5, 6), (0, 1))
    yrun(ystep, (1, 2), (2,))
    xforward(3)
    project_near(xfrom1, 1)
    wstep(4, 0)
    wstep(4, 1)


    xother = mod(x + 1 + 2 * c, NX)
    for k in range(XN):
        slot = xslot(xother, k)
        remote(slot, slot, xsend.at[0], xrecv.at[(1 - c) * XN + k], sib).wait_recv()
    project_near(xother, 2)
    wait_all(wb.at[0:384, :], 4)
    project_far(x, 0)
    yrun(ystep, (7,), (0, 1))
    ppair(1)
    yrun(pystep, (0,), (0, 1))
    yrun(ystep, (3, 4), (2,))
    project_far(xfrom1, 1)
    qpair(1)
    yrun(ystep, (5, 6), (2,))
    project_far(xother, 2)

    def xlast(k):
        slot = xslot(xfrom2, k)
        remote(slot, slot, xsend.at[0], xrecv.at[2 * XN + k], sib).wait_recv()

    for k in range(XN - 1):
        xlast(k)
    project(xfrom2, 0, ROWS - XR, (0, 1))
    ppair(2)
    yrun(ystep, (7,), (2,))
    project(xfrom2, 0, ROWS - XR, (1, 2))

    xlast(XN - 1)
    project(xfrom2, ROWS - XR, XR, (0, 1))

    for cc in range(2):
        @pl.when(c != cc)
        def _():
            wait_all(mb.at[:, 0:MSUM[cc], :], 0)

    kmax = (384, 640, 1024, 1280)
    kfree = (0, 256, 640, 896)

    def lanes(j, xx):
        return pl.ds(pl.multiple_of((4 * j + xx) * GD, GD), GD)

    def acopy(j, r):
        src = g.at[j, pl.ds(ROWS * r, ROWS), :]
        return remote(src, ab.at[:, lanes(j, x)], asend.at[0], arecv.at[j], dev(r, y, z, c))

    def alocal(j, r):
        src = g.at[j, pl.ds(ROWS * r, ROWS), :]
        return pltpu.make_async_copy(src, ab.at[:, lanes(j, x)], asem.at[0])

    def mix(j, _):
        for r in range(4):
            rows = pl.ds(ROWS * r, ROWS)
            k0, k1 = kfree[r], kmax[r]
            at_row = lax.broadcasted_iota(jnp.int32, (ROWS, k1 - k0), 0) + ROWS * r
            at_col = lax.broadcasted_iota(jnp.int32, (ROWS, k1 - k0), 1) + k0
            edge = mb[j, rows, k0:k1].astype(f32)
            edge = jnp.where(at_col <= at_row, edge, 0.0).astype(bf16)
            total = jnp.dot(edge, v[j, k0:k1, :], preferred_element_type=f32)
            if k0:
                total += jnp.dot(
                    mb[j, rows, 0:k0], v[j, 0:k0, :], preferred_element_type=f32
                )
            g[j, rows, :] = (op[j, rows, :] * (total + bt[j, rows, :])).astype(bf16)

        for r in range(4):
            @pl.when(x != r)
            def _():
                acopy(j, r).start()

            @pl.when(x == r)
            def _():
                alocal(j, r).start()
        return 0

    lax.fori_loop(0, 1, mix, 0)
    yrun(pystep, (1, 2), (0, 1))
    lax.fori_loop(1, 2, mix, 0)
    qstep(2, 0, 0)
    qstep(2, 0, 1)
    project(xfrom2, ROWS - XR, XR, (1, 2))
    lax.fori_loop(2, 3, mix, 0)
    ppair(3)
    qstep(2, 1, 0)
    qstep(2, 1, 1)
    yrun(pystep, (3, 4), (0, 1))
    lax.fori_loop(3, 4, mix, 0)
    pstep(4)
    qstep(3, 0, 0)
    qstep(3, 0, 1)
    qstep(3, 1, 0)
    qstep(3, 1, 1)
    yrun(pystep, (5, 6), (0, 1))
    yrun(pystep, (0, 1, 2), (2,))
    yrun(pystep, (7,), (0, 1))
    qstep(4, 0)
    yrun(pystep, (3, 4), (2,))
    qstep(4, 1)
    yrun(pystep, (5, 6), (2,))

    pltpu.make_async_copy(ab.at[:, 0:4 * GD], ab.at[:, 0:4 * GD], asem.at[0]).wait()

    def prepare(j):
        slot = ab.at[:, 0:3 * GD]
        remote(slot, slot, asend.at[0], arecv.at[j], sib).wait_recv()

        def piece(i, _):
            rows = pl.ds(pl.multiple_of(i * 64, 16), 64)
            squares = jnp.zeros((64, GD), f32)
            for k in range(512 * j, 512 * j + 512, GD):
                a = ab[rows, k:k + GD].astype(f32)
                squares += a * a
                nb[rows, k:k + GD] = (a * og[:, k:k + GD]).astype(bf16)
            if j:
                squares += ss[rows, :]
            ss[rows, :] = squares
            return 0

        lax.fori_loop(0, ROWS // 64, piece, 0)

    def partial_out(k0, k1):
        if k1 == WIDTH:
            mean = jnp.sum(ss[...], axis=-1, keepdims=True) * (1.0 / WIDTH)
            scale = lax.rsqrt(mean + norm_eps)

        def product(i, _):
            cols = pl.ds(pl.multiple_of(i * 1024, 1024), 1024)
            p = jnp.dot(nb[:, k0:k1], ob[k0:k1, cols], preferred_element_type=f32)
            if k0:
                p += acc[:, cols]
            if k1 < WIDTH:
                acc[:, cols] = p
            else:
                ov[:, cols] = (p * scale).astype(bf16)
                pltpu.make_async_copy(ov.at[:, cols], out_ref.at[0, :, cols], osem.at[0]).start()
            return 0

        lax.fori_loop(0, 2, product, 0)

    def msent(i, _):
        r, w = lax.div(i, 2), lax.rem(i, 2)
        org = mod(z + lax.select(w == 0, NZ - r, r), NZ)

        def go(width):
            slot = mslot(y, org * 2 + c, width)
            remote(slot, slot, zmsend.at[i], zmrecv.at[0], sib).wait_send()

        @pl.when((i < 6) | ((i == 6) & light[0]) | ((i == 7) & light[1]))
        def _():
            by_width(org * 2 + c, go)
        return 0

    lax.fori_loop(0, 8, msent, 0)
    prepare(0)
    prepare(1)
    wait_all(ob.at[0:OZ, 0:1024], 2)
    yrun(pystep, (7,), (2,))
    partial_out(0, KA)
    prepare(2)
    wait_all(ob.at[0:WIDTH - OZ, 0:1024], 3)
    partial_out(KA, 1536)
    prepare(3)
    partial_out(1536, WIDTH)

    def sent(ref, sem):
        remote(ref, ref, sem, brecv.at[0], sib).wait_send()

    sent(sb.at[0:3], ssend.at[0])
    sent(sg.at[0:3], ssend.at[1])
    sent(tok.at[0:3], xsend.at[0])
    sent(wb.at[0:768, :], zwsend.at[0])
    for w in range(2):
        @pl.when(light[w])
        def _():
            sent(wb.at[0:GD, :], zwsend.at[1 + w])
    sent(ob.at[0:OZ, 0:896], zqsend.at[0])
    sent(ob.at[0:OQ, 0:896], zpsend.at[0])
    sent(ob.at[0:OQ * 2, 0:1536], oysend.at[0])
    sent(wb.at[0:1024, :], bsend.at[1])
    sent(ob.at[0:OZ, 0:1024], bsend.at[2])
    sent(ob.at[0:WIDTH - OZ, 0:1024], bsend.at[3])
    sent(ab.at[:, 0:12 * GD], asend.at[0])
    for cc in range(2):
        @pl.when(c == cc)
        def _():
            sent(mb.at[:, 0:MSUM[cc], :], bsend.at[0])
            sent(mb.at[0:3, 0:MSUM[cc], :], ysend.at[0])

    pltpu.make_async_copy(ov, out_ref.at[0], osem.at[0]).wait()


def body(tokens, up_weight, gate_weight, group_gain, mix_weight, mix_bias, out_gain, out_weight):
    hbm = pl.BlockSpec(memory_space=pltpu.HBM)
    dma = pltpu.SemaphoreType.DMA
    return pl.pallas_call(
        kernel,
        out_shape=jax.ShapeDtypeStruct((1, ROWS, WIDTH), bf16),
        in_specs=[hbm] * 8,
        out_specs=pl.BlockSpec(memory_space=pl.ANY),
        scratch_shapes=[
            pltpu.VMEM((NX, ROWS, WIDTH), bf16),
            pltpu.VMEM((WIDTH, 1024), bf16),
            pltpu.VMEM((4, SPAN, SPAN), bf16),
            pltpu.VMEM((WIDTH, WIDTH), bf16),
            pltpu.VMEM((4, SPAN, GD), bf16),
            pltpu.VMEM((4, SPAN, GD), f32),
            pltpu.VMEM((4, SPAN, GD), f32),
            pltpu.VMEM((4, SPAN, GD), bf16),
            pltpu.VMEM((ROWS, WIDTH), bf16),
            pltpu.VMEM((ROWS, WIDTH), bf16),
            pltpu.VMEM((4, 1, SPAN), f32),
            pltpu.VMEM((4, 1, GD), f32),
            dma((7,)),
            dma((1,)),
            dma((12,)),
            dma((8,)),
            dma((8,)),
            dma((3,)),
            dma((16,)),
            dma((1,)),
            dma((16,)),
            dma((1,)),
            dma((8,)),
            dma((1,)),
            dma((24,)),
            dma((1,)),
            dma((24,)),
            dma((4,)),
            dma((5,)),
            dma((1,)),
            dma((4,)),
            dma((2,)),
            dma((2,)),
            dma((1,)),
            dma((1,)),
            pltpu.VMEM((ROWS, WIDTH), bf16),
            pltpu.VMEM((1, WIDTH), f32),
            pltpu.VMEM((ROWS, WIDTH), f32),
            pltpu.VMEM((ROWS, GD), f32),
            pltpu.VMEM((3, ROWS, 1024), f32),
        ],
        compiler_params=pltpu.CompilerParams(
            collective_id=0, has_side_effects=True, vmem_limit_bytes=54_000_000
        ),
        name="gating",
    )(
        *(
            pltpu.with_memory_space_constraint(a, pltpu.HBM)
            for a in (
                tokens, up_weight, gate_weight, group_gain, mix_weight, mix_bias,
                out_gain.reshape(1, WIDTH), out_weight,
            )
        )
    )


def solution(mesh):
    return jax.shard_map(
        body,
        mesh=mesh,
        in_specs=(
            P("dp", "sp", None),
            P("dp", None),
            P("dp", None),
            P("sp", None),
            P("sp", "dp", None),
            P("sp", None),
            P(),
            P(None, "dp"),
        ),
        out_specs=P("dp", "sp", None),
        check_vma=False,
    )
```
